1024 devices in a mesh: tp: 64 (over z, y), dp: 16 (over x, core).
Axes of the slice: x: 8, y: 8, z: 8, core: 2. Of those that a mesh axis runs over, the one named last changes fastest.
Arguments:
- stream: bfloat16 [128, 4096], P('dp', 'tp'), may hold values from -6 to 6
- query_weight: bfloat16 [2, 4096, 3072], P(None, 'dp', 'tp'), may hold values from -0.09375 to 0.09375
- key_weight: bfloat16 [2, 4096, 3072], P(None, 'dp', 'tp'), may hold values from -0.09375 to 0.09375
- value_weight: bfloat16 [2, 4096, 3072], P(None, 'dp', 'tp'), may hold values from -0.09375 to 0.09375
- outgate_weight: bfloat16 [2, 4096, 3072], P(None, 'dp', 'tp'), may hold values from -0.09375 to 0.09375
- gate_weight: bfloat16 [2, 4096, 32], replicated, may hold values from -0.09375 to 0.09375
- gate_bias: float32 [2, 32], replicated, may hold values from -1 to 3
- output_weight: bfloat16 [2, 3072, 4096], P(None, 'dp', 'tp'), may hold values from -0.109375 to 0.109375
- norm_gain: float32 [2, 4096], replicated, may hold values from 0.1 to 1.9
- matrix_state: float32 [2, 128, 192, 16, 192], P(None, 'dp', 'tp'), may hold values from -0.6 to 0.6
- normalizer_state: float32 [2, 128, 16, 192], P(None, 'dp'), may hold values from -0.6 to 0.6
- stabilizer_state: float32 [2, 128, 16], P(None, 'dp'), may hold values from -4 to 4
Outputs:
- out_stream: bfloat16 [128, 4096], P('dp', 'tp')
- new_matrix: float32 [2, 128, 192, 16, 192], P(None, 'dp', 'tp')
- new_normalizer: float32 [2, 128, 16, 192], P(None, 'dp')
- new_stabilizer: float32 [2, 128, 16], P(None, 'dp')
The draws below stay inside these ranges and needn't reach their ends.
All inputs are finite; a program needn't handle non-finite values.
Results may differ from the reference program's by a relative error of at most 0.015.
Values may be sent and summed in bfloat16 or wider, within the bound.
No kernel may reach another device: no remote copies, remote signals or barrier semaphores. Data moves between devices by JAX's collectives and lax.ppermute only.
A program may use at most 32 MiB of HBM per device.

```python
import jax
import jax.numpy as jnp
from jax import lax

D = 4096
HEADS = 16
HEAD_DIM = 192
BLOCKS = 2
SEQS = 128
VALUE_WIDTH = 3072


def steps_of(key, shape, shards, smallest, high):
    def one(axis_at, blocks):
        steps = jax.random.uniform(jax.random.fold_in(jax.random.fold_in(key, 6), axis_at), (blocks,), jnp.float32, smallest / len(shards), high / len(shards))
        return jnp.repeat(jnp.exp(steps), shape[axis_at] // blocks).reshape((-1,) + (1,) * (len(shape) - axis_at - 1))

    level = one(*shards[0])
    for cut in shards[1:]:
        level = level * one(*cut)
    return level


def scatter_about(key, dims, scale, reach, cuts=(), held_as=jnp.bfloat16):
    entries = jax.random.normal(key, dims, jnp.float32) * scale
    if len(cuts) > 0:
        entries = steps_of(key, dims, cuts, -0.22, 0.18) * entries
    return jnp.clip(entries, min=-reach, max=reach).astype(held_as)


def setup_inputs(seed: int = 0) -> dict:
    key_list = jax.random.split(jax.random.key(seed), 13)
    stream = scatter_about(key_list[0], (SEQS, D), 1.0, 6.0, ((0, 16), (1, 64)))
    query_weight = scatter_about(key_list[1], (BLOCKS, D, VALUE_WIDTH), D ** -0.5, 0.09375, ((1, 16), (2, 64)))
    key_weight = scatter_about(key_list[2], (BLOCKS, D, VALUE_WIDTH), D ** -0.5, 0.09375, ((1, 16), (2, 64)))
    value_weight = scatter_about(key_list[3], (BLOCKS, D, VALUE_WIDTH), D ** -0.5, 0.09375, ((1, 16), (2, 64)))
    outgate_weight = scatter_about(key_list[4], (BLOCKS, D, VALUE_WIDTH), D ** -0.5, 0.09375, ((1, 16), (2, 64)))
    gate_weight = scatter_about(key_list[5], (BLOCKS, D, 2 * HEADS), D ** -0.5, 0.09375)
    gate_bias = jnp.clip(jax.random.uniform(key_list[6], (BLOCKS, 2 * HEADS), jnp.float32, -1.0, 3.0), -1.0, 3.0)
    output_weight = scatter_about(key_list[7], (BLOCKS, VALUE_WIDTH, D), VALUE_WIDTH ** -0.5, 0.109375, ((1, 16), (2, 64)))
    norm_gain = jnp.clip(1.0 + 0.18 * jax.random.normal(key_list[8], (BLOCKS, D), jnp.float32), 0.1, 1.9)
    matrix_state = scatter_about(key_list[9], (BLOCKS, SEQS, HEAD_DIM, HEADS, HEAD_DIM), 0.1, 0.6, ((1, 16), (2, 64)), jnp.float32)
    normalizer_state = scatter_about(key_list[10], (BLOCKS, SEQS, HEADS, HEAD_DIM), 0.1, 0.6, ((1, 16),), jnp.float32)
    stabilizer_state = scatter_about(key_list[11], (BLOCKS, SEQS, HEADS), 1.0, 4.0, ((1, 16),), jnp.float32)
    return {"stream": stream, "query_weight": query_weight, "key_weight": key_weight, "value_weight": value_weight, "outgate_weight": outgate_weight, "gate_weight": gate_weight, "gate_bias": gate_bias, "output_weight": output_weight, "norm_gain": norm_gain, "matrix_state": matrix_state, "normalizer_state": normalizer_state, "stabilizer_state": stabilizer_state}


residual_scale = 8.0 ** 0.25
norm_eps = 1e-05

def normalize(values_in, gain):
    upcast = values_in.astype(jnp.float32)
    average = lax.optimization_barrier(jnp.mean(upcast, axis=-1, keepdims=True))
    variance = lax.optimization_barrier(jnp.mean(jnp.square(upcast - average), axis=-1, keepdims=True))
    return ((upcast - average) * lax.rsqrt(variance + norm_eps) * gain).astype(jnp.bfloat16)

def reference(stream, query_weight, key_weight, value_weight, outgate_weight, gate_weight, gate_bias, output_weight, norm_gain, matrix_state, normalizer_state, stabilizer_state):
    seq_count = stream.shape[0]
    current = stream
    new_mats, new_norms, new_stabs = ([], [], [])
    for block_no in range(BLOCKS):
        query = jnp.dot(current, query_weight[block_no], preferred_element_type=jnp.float32).astype(jnp.bfloat16)
        key_vec = jnp.dot(current, key_weight[block_no], preferred_element_type=jnp.float32).astype(jnp.bfloat16)
        value = jnp.dot(current, value_weight[block_no], preferred_element_type=jnp.float32).astype(jnp.bfloat16)
        outgate = jnp.dot(current, outgate_weight[block_no], preferred_element_type=jnp.float32).astype(jnp.bfloat16)
        gate_pre = jnp.dot(current, gate_weight[block_no], preferred_element_type=jnp.float32) + gate_bias[block_no]
        log_in = gate_pre[:, :HEADS]
        log_forget = jax.nn.log_sigmoid(gate_pre[:, HEADS:])
        old_stab = stabilizer_state[block_no]
        stab_new = jnp.maximum(log_forget + old_stab, log_in)
        retain = jnp.exp(log_forget + old_stab - stab_new)
        admit = jnp.exp(log_in - stab_new)
        queries = query.astype(jnp.float32).reshape(seq_count, HEADS, HEAD_DIM)
        keys = key_vec.astype(jnp.float32).reshape(seq_count, HEADS, HEAD_DIM) * HEAD_DIM ** (-0.5)
        values = value.astype(jnp.float32).reshape(seq_count, HEAD_DIM, HEADS)
        matrix = retain[:, None, :, None] * matrix_state[block_no] + admit[:, None, :, None] * values[..., None] * keys[:, None, :, :]
        norm_new = retain[..., None] * normalizer_state[block_no] + admit[..., None] * keys
        numerator = jnp.einsum('shd,sehd->seh', queries, matrix, precision=lax.Precision.HIGHEST)
        denominator = lax.optimization_barrier(jnp.sum(queries * norm_new, axis=-1))
        divisor = jnp.maximum(jnp.abs(denominator), 1.0)
        readout = (numerator / divisor[:, None, :]).reshape(seq_count, HEADS * HEAD_DIM)
        hidden = (readout * jax.nn.sigmoid(outgate.astype(jnp.float32))).astype(jnp.bfloat16)
        branch = jnp.dot(hidden, output_weight[block_no], preferred_element_type=jnp.float32)
        summed = (residual_scale * current.astype(jnp.float32) + branch).astype(jnp.bfloat16)
        current = normalize(summed, norm_gain[block_no])
        new_mats.append(matrix)
        new_norms.append(norm_new)
        new_stabs.append(stab_new)
    return (current, jnp.stack(new_mats), jnp.stack(new_norms), jnp.stack(new_stabs))
```

```python
import jax
import jax.numpy as jnp
from jax import lax
from jax.sharding import PartitionSpec as P

residual_scale = 8.0**0.25
norm_eps = 1e-05


def exchange(pieces, axis):
    return lax.all_to_all(pieces, axis, split_axis=0, concat_axis=0, tiled=True)


def collect(x, axis):
    return exchange(jnp.broadcast_to(x, (lax.axis_size(axis), *x.shape)), axis)


def collect_columns(x):
    pieces = collect(x, "tp")
    return jnp.moveaxis(pieces, 0, 1).reshape(x.shape[0], -1)


def double_up(block):
    held = block[None]
    size = lax.axis_size("dp")
    for bit in far_first(size):
        got = lax.ppermute(held, "dp", [(i, i ^ bit) for i in range(size)])
        held = jnp.concatenate([held, got])
    return held


def far_first(size):
    bits = []
    while size > 1:
        size //= 2
        bits.append(size)
    return bits


def order_like(x, rows):
    size = lax.axis_size("dp")
    me = lax.axis_index("dp")
    blocks = x.reshape(x.shape[0], size, rows)
    out = [blocks]
    cut = blocks
    bits = far_first(size)
    cut = cut.reshape(x.shape[0], *([2] * len(bits)), rows)
    for place, bit in enumerate(bits):
        flip = (me // bit) % 2
        axis = 1 + place
        cut = jnp.where(flip == 1, jnp.flip(cut, axis), cut)
    order = [0] + [1 + p for p in reversed(range(len(bits)))] + [1 + len(bits)]
    return jnp.transpose(cut, order).reshape(x.shape[0], size * rows)


def normalize(values_in, gain):
    upcast = values_in.astype(jnp.float32)
    average = jnp.mean(upcast, axis=-1, keepdims=True)
    variance = jnp.mean(jnp.square(upcast - average), axis=-1, keepdims=True)
    return ((upcast - average) * lax.rsqrt(variance + norm_eps) * gain).astype(jnp.bfloat16)


def shards(
    stream,
    query_weight,
    key_weight,
    value_weight,
    outgate_weight,
    gate_weight,
    gate_bias,
    output_weight,
    norm_gain,
    matrix_state,
    normalizer_state,
    stabilizer_state,
):
    head_count = gate_bias.shape[1] // 2
    head_size = normalizer_state.shape[3]
    seq_local = stream.shape[0]
    feat_local = stream.shape[1]
    row_local = query_weight.shape[1]
    col_local = query_weight.shape[2]
    out_rows = output_weight.shape[1]
    owners = lax.axis_size("dp")
    feat_offset = lax.axis_index("tp") * feat_local
    joined = jnp.concatenate([query_weight, key_weight, value_weight, outgate_weight], axis=2)

    out_first = double_up(output_weight[0]).reshape(owners * out_rows, feat_local)
    later = double_up(joined[1]).reshape(owners * row_local, 4 * col_local)
    out_second = double_up(output_weight[1]).reshape(owners * out_rows, feat_local)
    out_weights = (out_first, out_second)

    x_local = stream
    x_full = collect_columns(stream)
    new_mats, new_norms, new_stabs = ([], [], [])
    for block_no in range(gate_bias.shape[0]):
        if block_no == 0:
            pieces = jnp.moveaxis(x_full.reshape(seq_local, owners, row_local), 1, 0)
            everyone = exchange(pieces, "dp").reshape(owners * seq_local, row_local)
            partial = jnp.dot(everyone, joined[0], preferred_element_type=jnp.float32)
            partial = partial.astype(jnp.bfloat16).reshape(owners, seq_local, -1)
            packed = jnp.sum(exchange(partial, "dp").astype(jnp.float32), axis=0)
        else:
            packed = jnp.dot(
                order_like(x_full, row_local), later, preferred_element_type=jnp.float32
            )
        projected = packed.astype(jnp.bfloat16)
        value_part = projected[:, 2 * col_local : 3 * col_local]
        outgate_part = projected[:, 3 * col_local :]
        both = collect(projected[:, : 2 * col_local], "tp").reshape(-1, seq_local, 2, col_local)
        both = jnp.transpose(both, (2, 1, 0, 3)).reshape(2, seq_local, head_count, head_size)
        gate_pre = (
            jnp.dot(x_full, gate_weight[block_no], preferred_element_type=jnp.float32)
            + gate_bias[block_no]
        )
        log_in = gate_pre[:, :head_count]
        log_forget = jax.nn.log_sigmoid(gate_pre[:, head_count:])
        old_stab = stabilizer_state[block_no]
        stab_new = jnp.maximum(log_forget + old_stab, log_in)
        retain = jnp.exp(log_forget + old_stab - stab_new)
        admit = jnp.exp(log_in - stab_new)
        queries = both[0].astype(jnp.float32)
        keys = both[1].astype(jnp.float32) * head_size ** (-0.5)
        values = value_part.astype(jnp.float32).reshape(seq_local, -1, head_count)
        matrix = (
            retain[:, None, :, None] * matrix_state[block_no]
            + admit[:, None, :, None] * values[..., None] * keys[:, None, :, :]
        )
        norm_new = retain[..., None] * normalizer_state[block_no] + admit[..., None] * keys
        numerator = jnp.einsum("shd,sehd->seh", queries, matrix)
        denominator = jnp.sum(queries * norm_new, axis=-1)
        divisor = jnp.maximum(jnp.abs(denominator), 1.0)
        readout = (numerator / divisor[:, None, :]).reshape(seq_local, col_local)
        hidden = (readout * jax.nn.sigmoid(outgate_part.astype(jnp.float32))).astype(jnp.bfloat16)
        hidden_full = collect_columns(hidden)
        branch = jnp.dot(
            order_like(hidden_full, out_rows),
            out_weights[block_no],
            preferred_element_type=jnp.float32,
        )
        summed = (residual_scale * x_local.astype(jnp.float32) + branch).astype(jnp.bfloat16)
        x_full = normalize(collect_columns(summed), norm_gain[block_no])
        x_local = lax.dynamic_slice_in_dim(x_full, feat_offset, feat_local, 1)
        new_mats.append(matrix)
        new_norms.append(norm_new)
        new_stabs.append(stab_new)
    return (x_local, jnp.stack(new_mats), jnp.stack(new_norms), jnp.stack(new_stabs))


def solution(mesh):
    return jax.shard_map(
        shards,
        mesh=mesh,
        in_specs=(
            P("dp", "tp"),
            P(None, "dp", "tp"),
            P(None, "dp", "tp"),
            P(None, "dp", "tp"),
            P(None, "dp", "tp"),
            P(),
            P(),
            P(None, "dp", "tp"),
            P(),
            P(None, "dp", "tp", None, None),
            P(None, "dp", None, None),
            P(None, "dp", None),
        ),
        out_specs=(
            P("dp", "tp"),
            P(None, "dp", "tp", None, None),
            P(None, "dp", None, None),
            P(None, "dp", None),
        ),
        check_vma=False,
    )
```

```python
import functools

import jax
import jax.numpy as jnp
from jax import lax
from jax.experimental import pallas as pl
from jax.experimental.pallas import tpu as pltpu
from jax.sharding import PartitionSpec as P

residual_scale = 8.0**0.25
norm_eps = 1e-05


def collect(x, axis):
    copies = jnp.broadcast_to(x, (lax.axis_size(axis), *x.shape))
    return lax.all_to_all(copies, axis, split_axis=0, concat_axis=0, tiled=True)


def side_by_side(pieces):
    return jnp.moveaxis(pieces, 0, 1).reshape(pieces.shape[1], -1)


def after(x, earlier):
    return lax.optimization_barrier((x, *earlier))[0]


def step_of(held, bit):
    size = lax.axis_size("dp")
    return lax.ppermute(held, "dp", [(i, i ^ bit) for i in range(size)])


def merged(held, got):
    return lax.optimization_barrier(jnp.concatenate([held, got]))


def slots(size):
    held, bit = [0], size // 2
    while bit > 1:
        held = held + [h ^ bit for h in held]
        bit //= 2
    return held


def project_kernel(order, low, high, x_ref, held_ref, got_ref, out_ref):
    me = lax.axis_index("dp")
    rows = held_ref.shape[2]
    total = jnp.zeros(out_ref.shape, jnp.float32)
    for slot, other in enumerate(order):
        for half, ref in enumerate((held_ref, got_ref)):
            at = pl.multiple_of((me ^ (other ^ half)) * rows, rows)
            total = total + lax.dot_general(
                x_ref[:, pl.ds(at, rows)],
                ref[slot, low:high, :],
                (((1,), (1,)), ((), ())),
                preferred_element_type=jnp.float32,
            )
    out_ref[...] = total.astype(out_ref.dtype)


def project(x, halves, low, high, dtype):
    order = slots(lax.axis_size("dp"))
    flops = 2 * x.shape[0] * x.shape[1] * (high - low)
    return pl.pallas_call(
        functools.partial(project_kernel, order, low, high),
        out_shape=jax.ShapeDtypeStruct((x.shape[0], high - low), dtype),
        cost_estimate=pl.CostEstimate(
            flops=flops, bytes_accessed=2 * halves[0].size * 2, transcendentals=0
        ),
        compiler_params=pltpu.CompilerParams(vmem_limit_bytes=16 * 2**20),
        name="project",
    )(x, *halves)


def normalize(values_in, gain):
    upcast = values_in.astype(jnp.float32)
    average = jnp.mean(upcast, axis=-1, keepdims=True)
    variance = jnp.mean(jnp.square(upcast - average), axis=-1, keepdims=True)
    return ((upcast - average) * lax.rsqrt(variance + norm_eps) * gain).astype(jnp.bfloat16)


def shards(
    stream,
    query_weight,
    key_weight,
    value_weight,
    outgate_weight,
    gate_weight,
    gate_bias,
    output_weight,
    norm_gain,
    matrix_state,
    normalizer_state,
    stabilizer_state,
):
    head_count = gate_bias.shape[1] // 2
    head_size = normalizer_state.shape[3]
    seq_local = stream.shape[0]
    feat_local = stream.shape[1]
    row_local = query_weight.shape[1]
    col_local = query_weight.shape[2]
    feat_offset = lax.axis_index("tp") * feat_local
    per_block = row_local // feat_local
    turned = [jnp.swapaxes(w, 1, 2) for w in (query_weight, key_weight, value_weight, outgate_weight)]
    out_turned = jnp.swapaxes(output_weight, 1, 2).reshape(-1, feat_local, per_block, col_local)
    room = feat_local - col_local
    out_turned = jnp.pad(out_turned, ((0, 0), (0, 0), (0, 0), (0, room)))
    out_turned = out_turned.reshape(-1, feat_local, row_local)

    chain_a = jnp.concatenate([w[0] for w in turned[:2]])[None]
    chain_b = jnp.concatenate([w[0] for w in turned[2:]] + [out_turned[0]])[None]
    chain_c = jnp.concatenate([w[1] for w in turned] + [out_turned[1]])[None]

    got_a = step_of(chain_a, 8)
    x_local = stream
    x_full = side_by_side(collect(stream, "tp"))
    chain_a = merged(chain_a, got_a)
    got_a = step_of(chain_a, 4)
    got_b = step_of(after(chain_b, (chain_a,)), 8)
    chain_a = merged(chain_a, got_a)
    got_a = step_of(chain_a, 2)
    chain_b = merged(chain_b, got_b)
    got_b = step_of(after(chain_b, (chain_a,)), 4)
    chain_a = merged(chain_a, got_a)
    got_a = step_of(chain_a, 1)
    chain_b = merged(chain_b, got_b)
    new_mats, new_norms, new_stabs = ([], [], [])
    for block_no in range(gate_bias.shape[0]):
        if block_no == 0:
            qk = project(x_full, (chain_a, got_a), 0, 2 * col_local, jnp.bfloat16)
            got_b = step_of(chain_b, 2)
            got_c = step_of(after(chain_c, (qk,)), 8)
            chain_b = merged(chain_b, got_b)
            got_b = step_of(after(chain_b, (qk,)), 1)
            vo = project(x_full, (chain_b, got_b), 0, 2 * col_local, jnp.bfloat16)
            chain_c = merged(chain_c, got_c)
            got_c = step_of(after(chain_c, (qk,)), 4)
        else:
            qkvo = project(x_full, (chain_c, got_c), 0, 4 * col_local, jnp.bfloat16)
            qk, vo = qkvo[:, : 2 * col_local], qkvo[:, 2 * col_local :]
        value_part = vo[:, :col_local]
        outgate_part = vo[:, col_local:]
        both = collect(qk, "tp").reshape(-1, seq_local, 2, col_local)
        both = jnp.transpose(both, (2, 1, 0, 3)).reshape(2, seq_local, head_count, head_size)
        gate_pre = (
            jnp.dot(x_full, gate_weight[block_no], preferred_element_type=jnp.float32)
            + gate_bias[block_no]
        )
        log_in = gate_pre[:, :head_count]
        log_forget = jax.nn.log_sigmoid(gate_pre[:, head_count:])
        old_stab = stabilizer_state[block_no]
        stab_new = jnp.maximum(log_forget + old_stab, log_in)
        retain = jnp.exp(log_forget + old_stab - stab_new)
        admit = jnp.exp(log_in - stab_new)
        queries = both[0].astype(jnp.float32)
        keys = both[1].astype(jnp.float32) * head_size ** (-0.5)
        values = value_part.astype(jnp.float32).reshape(seq_local, -1, head_count)
        matrix = (
            retain[:, None, :, None] * matrix_state[block_no]
            + admit[:, None, :, None] * values[..., None] * keys[:, None, :, :]
        )
        norm_new = retain[..., None] * normalizer_state[block_no] + admit[..., None] * keys
        numerator = jnp.einsum("shd,sehd->seh", queries, matrix)
        denominator = jnp.sum(queries * norm_new, axis=-1)
        divisor = jnp.maximum(jnp.abs(denominator), 1.0)
        readout = (numerator / divisor[:, None, :]).reshape(seq_local, col_local)
        hidden = (readout * jax.nn.sigmoid(outgate_part.astype(jnp.float32))).astype(jnp.bfloat16)
        if block_no == 0:
            chain_c = merged(chain_c, got_c)
            got_c = step_of(after(chain_c, (hidden,)), 2)
        hidden_full = side_by_side(collect(jnp.pad(hidden, ((0, 0), (0, room))), "tp"))
        if block_no == 0:
            branch = project(
                hidden_full, (chain_b, got_b), 2 * col_local, 2 * col_local + feat_local, jnp.float32
            )
            chain_c = merged(chain_c, got_c)
            got_c = step_of(after(chain_c, (hidden_full,)), 1)
        else:
            branch = project(
                hidden_full, (chain_c, got_c), 4 * col_local, 4 * col_local + feat_local, jnp.float32
            )
        summed = (residual_scale * x_local.astype(jnp.float32) + branch).astype(jnp.bfloat16)
        x_full = normalize(side_by_side(collect(summed, "tp")), norm_gain[block_no])
        x_local = lax.dynamic_slice_in_dim(x_full, feat_offset, feat_local, 1)
        new_mats.append(matrix)
        new_norms.append(norm_new)
        new_stabs.append(stab_new)
    return (x_local, jnp.stack(new_mats), jnp.stack(new_norms), jnp.stack(new_stabs))


def solution(mesh):
    return jax.shard_map(
        shards,
        mesh=mesh,
        in_specs=(
            P("dp", "tp"),
            P(None, "dp", "tp"),
            P(None, "dp", "tp"),
            P(None, "dp", "tp"),
            P(None, "dp", "tp"),
            P(),
            P(),
            P(None, "dp", "tp"),
            P(),
            P(None, "dp", "tp", None, None),
            P(None, "dp", None, None),
            P(None, "dp", None),
        ),
        out_specs=(
            P("dp", "tp"),
            P(None, "dp", "tp", None, None),
            P(None, "dp", None, None),
            P(None, "dp", None),
        ),
        check_vma=False,
    )
```

```python
import functools

import jax
import jax.numpy as jnp
from jax import lax
from jax.experimental import pallas as pl
from jax.experimental.pallas import tpu as pltpu
from jax.sharding import PartitionSpec as P


residual_scale = 8.0**0.25
norm_eps = 1e-05
LANES = 128
F32 = jnp.float32


def exchange(pieces, axis, groups=None):
    return lax.all_to_all(
        pieces, axis, split_axis=0, concat_axis=0, tiled=True, axis_index_groups=groups
    )


def after(x, earlier):
    return lax.optimization_barrier((x, *earlier))[0]


def step_of(held, bit):
    size = lax.axis_size("dp")
    return lax.ppermute(held, "dp", [(i, i ^ bit) for i in range(size)])


def merged(held, got):
    return lax.optimization_barrier(jnp.concatenate([held, got]))


def chain_order(size):
    held, bit = [0], size // 2
    while bit > 1:
        held = held + [h ^ bit for h in held]
        bit //= 2
    return held


def row_dot(x, turned):
    return lax.dot_general(x, turned, (((1,), (1,)), ((), ())), preferred_element_type=F32)


def blocks_dot(x_ref, halves, order, whole, low, high):
    me = lax.axis_index("dp")
    base = me if whole else me & 1
    rows = halves[0].shape[2]
    total = jnp.zeros((x_ref.shape[0], high - low), F32)
    for slot, other in enumerate(order):
        for half, ref in enumerate(halves):
            at = pl.multiple_of((base ^ (other ^ half)) * rows, rows)
            total = total + row_dot(x_ref[:, pl.ds(at, rows)], ref[slot, low:high, :])
    return total


def pair_up(pieces_ref, width, at):
    two = [pieces_ref[2 * at + k][:, :width].astype(F32) for k in range(2)]
    return jnp.concatenate(two, axis=1)


def spread(ref, x):
    if x.shape[1] < LANES:
        x = jnp.concatenate([x, jnp.zeros((x.shape[0], LANES - x.shape[1]), x.dtype)], axis=1)
    x = x.astype(ref.dtype)
    for copy in range(ref.shape[0]):
        ref[copy] = x


def call(kernel, out_shape, *arrays, flops=10**6, scratch=()):
    moved = sum(a.size * a.dtype.itemsize for a in arrays)
    return pl.pallas_call(
        kernel,
        out_shape=out_shape,
        scratch_shapes=list(scratch),
        cost_estimate=pl.CostEstimate(flops=flops, bytes_accessed=moved, transcendentals=0),
        compiler_params=pltpu.CompilerParams(vmem_limit_bytes=20 * 2**20),
    )(*arrays)


def first_kernel(order, cut, high, pieces_ref, held_ref, got_ref, x_ref, qk_ref, vo_ref):
    width = x_ref.shape[1] // pieces_ref.shape[0]
    for at in range(pieces_ref.shape[0] // 2):
        cols = slice(2 * width * at, 2 * width * (at + 1))
        x_ref[:, cols] = pair_up(pieces_ref, width, at).astype(x_ref.dtype)
    out = blocks_dot(x_ref, (held_ref, got_ref), order, False, 0, high)
    spread(qk_ref, out[:, :cut])
    vo_ref[...] = out[:, cut:].astype(vo_ref.dtype)


def norm_kernel(order, cut, high, pieces_ref, gain_ref, held_ref, got_ref, x_ref, qk_ref, vo_ref):
    count, width = pieces_ref.shape[0], x_ref.shape[1] // pieces_ref.shape[0]
    pairs = [pair_up(pieces_ref, width, at) for at in range(count // 2)]
    features = x_ref.shape[1]
    mean = jnp.sum(sum(pairs), axis=1, keepdims=True) / features
    pairs = [p - mean for p in pairs]
    variance = jnp.sum(sum(p * p for p in pairs), axis=1, keepdims=True) / features
    scale = lax.rsqrt(variance + norm_eps)
    for at, p in enumerate(pairs):
        cols = slice(2 * width * at, 2 * width * (at + 1))
        x_ref[:, cols] = (p * scale * gain_ref[:, cols]).astype(x_ref.dtype)
    out = blocks_dot(x_ref, (held_ref, got_ref), order, True, 0, high)
    spread(qk_ref, out[:, :cut])
    vo_ref[...] = out[:, cut:].astype(vo_ref.dtype)


def head_sums(x, heads):
    x = x.reshape(heads, -1, *x.shape[1:]).sum(1)
    lane = lax.broadcasted_iota(jnp.int32, (x.shape[1], LANES), 1)
    sums = jnp.sum(x, axis=2, keepdims=True)
    total = jnp.zeros((x.shape[1], LANES), F32)
    for head in range(heads):
        total = jnp.where(lane == head, sums[head], total)
    return total


def readout_kernel(scale, pieces_ref, vo_ref, retain_ref, admit_ref, state_ref, normalizer_ref, out_ref):
    heads = retain_ref.shape[1]
    width = state_ref.shape[3]
    both = pieces_ref[...].astype(F32)
    query = both[:, :, :width]
    key = both[:, :, width : 2 * width] * scale
    retain, admit = retain_ref[...], admit_ref[...]
    of_key = head_sums(query * key, heads)[:, :heads] * admit
    of_normalizer = head_sums(query * normalizer_ref[...], heads)[:, :heads] * retain
    divisor = jnp.maximum(jnp.abs(of_normalizer + of_key), 1.0)
    vo = vo_ref[...].astype(F32)
    parts = []
    for e in range(state_ref.shape[0]):
        numerator = head_sums(query * state_ref[e], heads)[:, :heads] * retain
        value = vo[:, e * heads : (e + 1) * heads]
        gate = vo[:, width + e * heads : width + (e + 1) * heads]
        parts.append((numerator + value * of_key) / divisor * jax.nn.sigmoid(gate))
    spread(out_ref, jnp.concatenate(parts, axis=1))


def branch_kernel(order, whole, low, high, pieces_ref, x_ref, held_ref, got_ref, out_ref, wide_ref):
    width = high - low
    for at in range(pieces_ref.shape[0] // 2):
        cols = slice(2 * width * at, 2 * width * (at + 1))
        wide_ref[:, cols] = pair_up(pieces_ref, width, at).astype(wide_ref.dtype)
    branch = blocks_dot(wide_ref, (held_ref, got_ref), order, whole, low, high)
    spread(out_ref, residual_scale * x_ref[...].astype(F32) + branch)


def last_kernel(features, pieces_ref, gain_ref, out_ref):
    width = out_ref.shape[1]
    pieces = [pieces_ref[at].astype(F32) for at in range(pieces_ref.shape[0])]
    mean = jnp.sum(sum(pieces), axis=1, keepdims=True) / features
    lane = lax.broadcasted_iota(jnp.int32, pieces[0].shape, 1)
    off = [jnp.where(lane < width, p - mean, 0.0) for p in pieces]
    variance = jnp.sum(sum(p * p for p in off), axis=1, keepdims=True) / features
    own = pieces_ref[lax.axis_index("tp")].astype(F32)[:, :width]
    out = (own - mean) * lax.rsqrt(variance + norm_eps) * gain_ref[...]
    out_ref[...] = out.astype(out_ref.dtype)


def update(retain, admit, values, keys, state):
    fresh = admit[:, None, :, None] * values[..., None] * keys[:, None, :, :]
    return retain[:, None, :, None] * state + fresh


def shards(
    stream,
    query_weight,
    key_weight,
    value_weight,
    outgate_weight,
    gate_weight,
    gate_bias,
    output_weight,
    norm_gain,
    matrix_state,
    normalizer_state,
    stabilizer_state,
):
    head_count = gate_bias.shape[1] // 2
    head_size = normalizer_state.shape[3]
    seqs, feats = stream.shape
    rows, cols = query_weight.shape[1:]
    peers = lax.axis_size("tp")
    owners = lax.axis_size("dp")
    order = chain_order(owners)
    by_chip = [2 * chip for chip in range(owners // 2)]
    me = lax.axis_index("tp")
    bf16 = stream.dtype
    copies = jax.ShapeDtypeStruct((peers, seqs, LANES), bf16)
    pair = jax.ShapeDtypeStruct((seqs, 2 * cols), bf16)
    per_head = head_size // cols
    turned = [jnp.swapaxes(w, 1, 2) for w in (query_weight, key_weight, value_weight, outgate_weight)]
    out_turned = jnp.swapaxes(output_weight, 1, 2).reshape(-1, feats, rows // feats, cols)
    out_turned = jnp.pad(out_turned, ((0, 0), (0, 0), (0, 0), (0, feats - cols)))
    out_turned = out_turned.reshape(-1, feats, rows)

    bulk = jnp.concatenate([w[0] for w in turned])
    chain_d = out_turned[:1]
    chain_c = jnp.concatenate([w[1] for w in turned] + [out_turned[1]])[None]

    def by_piece(x):
        x = x.reshape(*x.shape[:-1], per_head, cols)
        return jnp.moveaxis(x, 0, -2).reshape(*x.shape[1:-3], peers, seqs, cols)

    states = [by_piece(m) for m in matrix_state]
    normalizers = [by_piece(n) for n in normalizer_state]

    chips = [[2 * chip + core for chip in range(owners // 2)] for core in range(2)]
    bulk = jnp.broadcast_to(bulk, (owners // 2, *bulk.shape))
    bulk = exchange(bulk, "dp", chips)
    tile = jnp.pad(stream, ((0, 0), (0, LANES - feats)))
    tile = after(tile, (*states, *normalizers, bulk))
    pieces = exchange(jnp.broadcast_to(tile, copies.shape), "tp")
    got_bulk = step_of(bulk, 1)
    got_d = step_of(chain_d, 8)
    got_c = step_of(chain_c, 8)
    x_local = stream
    whole_x = jax.ShapeDtypeStruct((seqs, peers * feats), bf16)
    saved, new_mats, new_norms, new_stabs = ([], [], [], [])
    for block_no in range(gate_bias.shape[0]):
        if block_no == 0:
            x_full, qk, vo = call(
                functools.partial(first_kernel, by_chip, 2 * cols, 4 * cols),
                (whole_x, copies, pair),
                pieces,
                bulk,
                got_bulk,
            )
            chain_d = merged(after(chain_d, (qk,)), got_d)
            got_d = step_of(chain_d, 4)
            chain_c = merged(after(chain_c, (qk,)), got_c)
            got_c = step_of(chain_c, 4)
        else:
            x_full, qk, vo = call(
                functools.partial(norm_kernel, order, 2 * cols, 4 * cols),
                (whole_x, copies, pair),
                pieces,
                norm_gain[:1],
                chain_c,
                got_c,
            )
            x_local = lax.dynamic_slice_in_dim(x_full, me * feats, feats, 1)
            saved[0] = (*saved[0][:4], qk)
        pieces = exchange(qk, "tp")
        gate_pre = (
            jnp.dot(x_full, gate_weight[block_no], preferred_element_type=F32)
            + gate_bias[block_no]
        )
        log_in = gate_pre[:, :head_count]
        log_forget = jax.nn.log_sigmoid(gate_pre[:, head_count:])
        old_stab = stabilizer_state[block_no]
        stab_new = jnp.maximum(log_forget + old_stab, log_in)
        retain = jnp.exp(log_forget + old_stab - stab_new)
        admit = jnp.exp(log_in - stab_new)
        hidden = call(
            functools.partial(readout_kernel, head_size**-0.5),
            copies,
            pieces,
            vo,
            retain,
            admit,
            states[block_no],
            normalizers[block_no],
        )
        if block_no == 0:
            chain_d = merged(after(chain_d, (hidden,)), got_d)
            got_d = step_of(chain_d, 2)
            chain_d = merged(chain_d, got_d)
            got_d = step_of(chain_d, 1)
            chain_c = merged(after(chain_c, (hidden,)), got_c)
            got_c = step_of(chain_c, 2)
        out_halves, out_low = ((chain_d, got_d), 0) if block_no == 0 else ((chain_c, got_c), 4 * cols)
        key_pieces = pieces[:, :, cols : 2 * cols]
        saved.append((key_pieces, vo, retain, admit, hidden))
        pieces = exchange(hidden, "tp")
        summed = call(
            functools.partial(branch_kernel, order, True, out_low, out_low + feats),
            copies,
            pieces,
            x_local,
            *out_halves,
            scratch=[pltpu.VMEM((seqs, peers * feats), bf16)],
        )
        if block_no == 0:
            chain_c = merged(after(chain_c, (summed,)), got_c)
            got_c = step_of(chain_c, 1)
        new_stabs.append(stab_new)
        pieces = exchange(summed, "tp")
    gain = lax.dynamic_slice_in_dim(norm_gain[1:], me * feats, feats, 1)
    out = call(
        functools.partial(last_kernel, peers * feats),
        jax.ShapeDtypeStruct((seqs, feats), bf16),
        pieces,
        gain,
    )
    for (key_pieces, vo, retain, admit, earlier), matrix, normalizer in zip(
        saved, matrix_state, normalizer_state
    ):
        keys = after(key_pieces, (earlier,))
        keys = jnp.moveaxis(keys, 0, 1).reshape(seqs, head_count, head_size).astype(F32)
        keys = keys * head_size ** (-0.5)
        values = vo[:, :cols].astype(F32).reshape(seqs, -1, head_count)
        new_mats.append(update(retain, admit, values, keys, matrix))
        new_norms.append(retain[..., None] * normalizer + admit[..., None] * keys)
    return (out, jnp.stack(new_mats), jnp.stack(new_norms), jnp.stack(new_stabs))


def solution(mesh):
    return jax.shard_map(
        shards,
        mesh=mesh,
        in_specs=(
            P("dp", "tp"),
            P(None, "dp", "tp"),
            P(None, "dp", "tp"),
            P(None, "dp", "tp"),
            P(None, "dp", "tp"),
            P(),
            P(),
            P(None, "dp", "tp"),
            P(),
            P(None, "dp", "tp", None, None),
            P(None, "dp", None, None),
            P(None, "dp", None),
        ),
        out_specs=(
            P("dp", "tp"),
            P(None, "dp", "tp", None, None),
            P(None, "dp", None, None),
            P(None, "dp", None),
        ),
        check_vma=False,
    )
```

```python
import functools

import jax
import jax.numpy as jnp
from jax import lax
from jax.experimental import pallas as pl
from jax.experimental.pallas import tpu as pltpu
from jax.sharding import PartitionSpec as P


residual_scale = 8.0**0.25
norm_eps = 1e-05
LANES = 128
F32 = jnp.float32


def exchange(pieces, axis, groups=None):
    return lax.all_to_all(
        pieces, axis, split_axis=0, concat_axis=0, tiled=True, axis_index_groups=groups
    )


def after(x, earlier):
    return lax.optimization_barrier((x, earlier))[0]


def step_of(held, bit):
    size = lax.axis_size("dp")
    return lax.ppermute(held, "dp", [(i, i ^ bit) for i in range(size)])


def merged(held, got):
    return lax.optimization_barrier(jnp.concatenate([held, got]))


def chain_order(size):
    held, bit = [0], size // 2
    while bit > 1:
        held = held + [h ^ bit for h in held]
        bit //= 2
    return held


def row_dot(x, turned):
    return lax.dot_general(x, turned, (((1,), (1,)), ((), ())), preferred_element_type=F32)


def blocks_dot(x_ref, halves, order, whole, low, high):
    me = lax.axis_index("dp")
    base = me if whole else me & 1
    rows = halves[0].shape[2]
    total = jnp.zeros((x_ref.shape[0], high - low), F32)
    for slot, other in enumerate(order):
        for half, ref in enumerate(halves):
            at = pl.multiple_of((base ^ (other ^ half)) * rows, rows)
            total = total + row_dot(x_ref[:, pl.ds(at, rows)], ref[slot, low:high, :])
    return total


def pair_up(pieces_ref, width, at):
    two = [pieces_ref[2 * at + k][:, :width].astype(F32) for k in range(2)]
    return jnp.concatenate(two, axis=1)


def spread(ref, x):
    if x.shape[1] < LANES:
        x = jnp.concatenate([x, jnp.zeros((x.shape[0], LANES - x.shape[1]), x.dtype)], axis=1)
    x = x.astype(ref.dtype)
    for copy in range(ref.shape[0]):
        ref[copy] = x


def call(kernel, out_shape, *arrays, flops=10**6, scratch=(), specs=None, out_specs=None, aliases=None):
    moved = sum(a.size * a.dtype.itemsize for a in arrays)
    extra = {} if specs is None else {"in_specs": specs, "grid": (1,)}
    if out_specs is not None:
        extra["out_specs"] = out_specs
    return pl.pallas_call(
        kernel,
        out_shape=out_shape,
        scratch_shapes=list(scratch),
        input_output_aliases=aliases or {},
        cost_estimate=pl.CostEstimate(flops=flops, bytes_accessed=moved, transcendentals=0),
        compiler_params=pltpu.CompilerParams(vmem_limit_bytes=32 * 2**20),
        **extra,
    )(*arrays)


def one_block(shape, at=None):
    at = at or (0,) * len(shape)
    return pl.BlockSpec(shape, lambda step: at)


def first_kernel(order, cut, high, pieces_ref, held_ref, got_ref, x_ref, qk_ref, vo_ref):
    width = x_ref.shape[1] // pieces_ref.shape[0]
    for at in range(pieces_ref.shape[0] // 2):
        cols = slice(2 * width * at, 2 * width * (at + 1))
        x_ref[:, cols] = pair_up(pieces_ref, width, at).astype(x_ref.dtype)
    out = blocks_dot(x_ref, (held_ref, got_ref), order, False, 0, high)
    spread(qk_ref, out[:, :cut])
    vo_ref[...] = out[:, cut:].astype(vo_ref.dtype)


def norm_kernel(order, cut, high, pieces_ref, gain_ref, held_ref, got_ref, x_ref, qk_ref, vo_ref):
    count, width = pieces_ref.shape[0], x_ref.shape[1] // pieces_ref.shape[0]
    pairs = [pair_up(pieces_ref, width, at) for at in range(count // 2)]
    features = x_ref.shape[1]
    mean = jnp.sum(sum(pairs), axis=1, keepdims=True) / features
    pairs = [p - mean for p in pairs]
    variance = jnp.sum(sum(p * p for p in pairs), axis=1, keepdims=True) / features
    scale = lax.rsqrt(variance + norm_eps)
    for at, p in enumerate(pairs):
        cols = slice(2 * width * at, 2 * width * (at + 1))
        x_ref[:, cols] = (p * scale * gain_ref[:, cols]).astype(x_ref.dtype)
    out = blocks_dot(x_ref, (held_ref, got_ref), order, True, 0, high)
    spread(qk_ref, out[:, :cut])
    vo_ref[...] = out[:, cut:].astype(vo_ref.dtype)


def head_sums(x, heads):
    x = x.reshape(heads, -1, *x.shape[1:]).sum(1)
    lane = lax.broadcasted_iota(jnp.int32, (x.shape[1], LANES), 1)
    sums = jnp.sum(x, axis=2, keepdims=True)
    total = jnp.zeros((x.shape[1], LANES), F32)
    for head in range(heads):
        total = jnp.where(lane == head, sums[head], total)
    return total


def readout_kernel(scale, pieces_ref, vo_ref, retain_ref, admit_ref, state_ref, normalizer_ref, out_ref):
    heads = retain_ref.shape[1]
    width = state_ref.shape[3]
    both = pieces_ref[...].astype(F32)
    query = both[:, :, :width]
    key = both[:, :, width : 2 * width] * scale
    retain, admit = retain_ref[...], admit_ref[...]
    of_key = head_sums(query * key, heads)[:, :heads] * admit
    of_normalizer = head_sums(query * normalizer_ref[...], heads)[:, :heads] * retain
    divisor = jnp.maximum(jnp.abs(of_normalizer + of_key), 1.0)
    vo = vo_ref[...].astype(F32)
    parts = []
    for e in range(state_ref.shape[0]):
        numerator = head_sums(query * state_ref[e], heads)[:, :heads] * retain
        value = vo[:, e * heads : (e + 1) * heads]
        gate = vo[:, width + e * heads : width + (e + 1) * heads]
        parts.append((numerator + value * of_key) / divisor * jax.nn.sigmoid(gate))
    spread(out_ref, jnp.concatenate(parts, axis=1))


def branch_kernel(order, whole, low, high, pieces_ref, x_ref, held_ref, got_ref, out_ref, wide_ref):
    width = high - low
    for at in range(pieces_ref.shape[0] // 2):
        cols = slice(2 * width * at, 2 * width * (at + 1))
        wide_ref[:, cols] = pair_up(pieces_ref, width, at).astype(wide_ref.dtype)
    branch = blocks_dot(wide_ref, (held_ref, got_ref), order, whole, low, high)
    spread(out_ref, residual_scale * x_ref[...].astype(F32) + branch)


def last_kernel(features, pieces_ref, gain_ref, out_ref):
    width = out_ref.shape[1]
    pieces = [pieces_ref[at].astype(F32) for at in range(pieces_ref.shape[0])]
    mean = jnp.sum(sum(pieces), axis=1, keepdims=True) / features
    lane = lax.broadcasted_iota(jnp.int32, pieces[0].shape, 1)
    off = [jnp.where(lane < width, p - mean, 0.0) for p in pieces]
    variance = jnp.sum(sum(p * p for p in off), axis=1, keepdims=True) / features
    own = pieces_ref[lax.axis_index("tp")].astype(F32)[:, :width]
    out = (own - mean) * lax.rsqrt(variance + norm_eps) * gain_ref[...]
    out_ref[...] = out.astype(out_ref.dtype)


def column(row, heads):
    at = lax.broadcasted_iota(jnp.int32, (heads, heads), 0)
    lane = lax.broadcasted_iota(jnp.int32, (heads, heads), 1)
    wide = jnp.broadcast_to(row, (heads, heads))
    return jnp.sum(jnp.where(at == lane, wide, 0.0), axis=1, keepdims=True)


def update_kernel(scale, parts, *refs):
    pieces_ref, vo_ref, retain_ref, admit_ref, state_ref, normalizer_ref = refs[:6]
    new_state_ref, new_normalizer_ref, rows_ref = refs[-3:]
    _, seqs, channels, heads, size = state_ref.shape
    width = size // parts
    rows_ref[...] = pieces_ref[...].astype(F32).reshape(rows_ref.shape)
    vo = vo_ref[...].astype(F32)
    for seq in range(seqs):
        found = [
            rows_ref[pl.ds(seq + seqs * part, heads, stride=seqs * parts), :]
            for part in range(parts)
        ]
        key = jnp.concatenate([f[:, width : 2 * width] for f in found], axis=1) * scale
        retain = column(retain_ref[seq : seq + 1, :], heads)
        admit = column(admit_ref[seq : seq + 1, :], heads)
        new_normalizer_ref[0, seq] = retain * normalizer_ref[0, seq] + admit * key
        for e in range(channels):
            value = column(vo[seq : seq + 1, e * heads : (e + 1) * heads], heads)
            new_state_ref[0, seq, e] = retain * state_ref[0, seq, e] + (admit * value) * key


def update(block_no, saved, state, normalizer, made):
    size, width = state.shape[4], saved[1].shape[1] // 2
    blocks = [
        one_block((1, *x.shape[1:]), (block_no,) + (0,) * (x.ndim - 1)) for x in (state, normalizer)
    ]
    whole = [one_block(x.shape) for x in saved]
    arrays = (*saved, state, normalizer, *made)
    return call(
        functools.partial(update_kernel, size**-0.5, size // width),
        [jax.ShapeDtypeStruct(x.shape, x.dtype) for x in (state, normalizer)],
        *arrays,
        scratch=[pltpu.VMEM((saved[0].shape[0] * saved[0].shape[1], LANES), F32)],
        specs=[*whole, *blocks, *[pl.BlockSpec(memory_space=pl.ANY) for _ in made]],
        out_specs=blocks,
        aliases={6: 0, 7: 1} if made else None,
    )


def shards(
    stream,
    query_weight,
    key_weight,
    value_weight,
    outgate_weight,
    gate_weight,
    gate_bias,
    output_weight,
    norm_gain,
    matrix_state,
    normalizer_state,
    stabilizer_state,
):
    head_count = gate_bias.shape[1] // 2
    head_size = normalizer_state.shape[3]
    seqs, feats = stream.shape
    rows, cols = query_weight.shape[1:]
    peers = lax.axis_size("tp")
    owners = lax.axis_size("dp")
    order = chain_order(owners)
    by_chip = [2 * chip for chip in range(owners // 2)]
    me = lax.axis_index("tp")
    bf16 = stream.dtype
    copies = jax.ShapeDtypeStruct((peers, seqs, LANES), bf16)
    pair = jax.ShapeDtypeStruct((seqs, 2 * cols), bf16)
    per_head = head_size // cols
    turned = [jnp.swapaxes(w, 1, 2) for w in (query_weight, key_weight, value_weight, outgate_weight)]
    out_turned = jnp.swapaxes(output_weight, 1, 2).reshape(-1, feats, rows // feats, cols)
    out_turned = jnp.pad(out_turned, ((0, 0), (0, 0), (0, 0), (0, feats - cols)))
    out_turned = out_turned.reshape(-1, feats, rows)

    bulk = jnp.concatenate([w[0] for w in turned])
    chain = jnp.concatenate([w[1] for w in turned] + [out_turned[0], out_turned[1]])[None]

    def by_piece(x):
        x = x.reshape(*x.shape[:-1], per_head, cols)
        return jnp.moveaxis(x, 0, -2).reshape(*x.shape[1:-3], peers, seqs, cols)

    states = [by_piece(m) for m in matrix_state]
    normalizers = [by_piece(n) for n in normalizer_state]

    chips = [[2 * chip + core for chip in range(owners // 2)] for core in range(2)]
    bulk = jnp.broadcast_to(bulk, (owners // 2, *bulk.shape))
    bulk = exchange(bulk, "dp", chips)
    got = step_of(chain, 8)
    tile = jnp.pad(stream, ((0, 0), (0, LANES - feats)))
    tile = after(tile, (*states, *normalizers, bulk))
    pieces = exchange(jnp.broadcast_to(tile, copies.shape), "tp")
    got_bulk = step_of(bulk, 1)
    chain = merged(after(chain, (bulk,)), got)
    got = step_of(chain, 4)
    x_local = stream
    whole_x = jax.ShapeDtypeStruct((seqs, peers * feats), bf16)
    saved, new_stabs = ([], [])
    for block_no in range(gate_bias.shape[0]):
        if block_no == 0:
            x_full, qk, vo = call(
                functools.partial(first_kernel, by_chip, 2 * cols, 4 * cols),
                (whole_x, copies, pair),
                pieces,
                bulk,
                got_bulk,
            )
            chain = merged(after(chain, (qk,)), got)
            got = step_of(chain, 2)
        else:
            halves = one_block((owners // 2, 4 * cols, rows))
            x_full, qk, vo = call(
                functools.partial(norm_kernel, order, 2 * cols, 4 * cols),
                (whole_x, copies, pair),
                pieces,
                norm_gain[:1],
                chain,
                got,
                specs=[one_block(pieces.shape), one_block((1, peers * feats)), halves, halves],
            )
            x_local = lax.dynamic_slice_in_dim(x_full, me * feats, feats, 1)
            tied = after(saved[0], (qk,))
            made = update(0, tied, matrix_state, normalizer_state, ())
        pieces = exchange(qk, "tp")
        gate_pre = (
            jnp.dot(x_full, gate_weight[block_no], preferred_element_type=F32)
            + gate_bias[block_no]
        )
        log_in = gate_pre[:, :head_count]
        log_forget = jax.nn.log_sigmoid(gate_pre[:, head_count:])
        old_stab = stabilizer_state[block_no]
        stab_new = jnp.maximum(log_forget + old_stab, log_in)
        retain = jnp.exp(log_forget + old_stab - stab_new)
        admit = jnp.exp(log_in - stab_new)
        hidden = call(
            functools.partial(readout_kernel, head_size**-0.5),
            copies,
            pieces,
            vo,
            retain,
            admit,
            states[block_no],
            normalizers[block_no],
        )
        if block_no == 0:
            chain = merged(after(chain, (hidden,)), got)
            got = step_of(chain, 1)
        saved.append((pieces, vo, retain, admit))
        pieces = exchange(hidden, "tp")
        halves = one_block((owners // 2, feats, rows), (0, 4 * cols // feats + block_no, 0))
        summed = call(
            functools.partial(branch_kernel, order, True, 0, feats),
            copies,
            pieces,
            x_local,
            chain,
            got,
            scratch=[pltpu.VMEM((seqs, peers * feats), bf16)],
            specs=[one_block(pieces.shape), one_block(x_local.shape), halves, halves],
        )
        new_stabs.append(stab_new)
        pieces = exchange(summed, "tp")
    gain = lax.dynamic_slice_in_dim(norm_gain[1:], me * feats, feats, 1)
    out = call(
        functools.partial(last_kernel, peers * feats),
        jax.ShapeDtypeStruct((seqs, feats), bf16),
        pieces,
        gain,
    )
    made = update(1, after(saved[1], (summed,)), matrix_state, normalizer_state, made)
    return (out, *made, jnp.stack(new_stabs))


def solution(mesh):
    return jax.shard_map(
        shards,
        mesh=mesh,
        in_specs=(
            P("dp", "tp"),
            P(None, "dp", "tp"),
            P(None, "dp", "tp"),
            P(None, "dp", "tp"),
            P(None, "dp", "tp"),
            P(),
            P(),
            P(None, "dp", "tp"),
            P(),
            P(None, "dp", "tp", None, None),
            P(None, "dp", None, None),
            P(None, "dp", None),
        ),
        out_specs=(
            P("dp", "tp"),
            P(None, "dp", "tp", None, None),
            P(None, "dp", None, None),
            P(None, "dp", None),
        ),
        check_vma=False,
    )
```

```python
import functools

import jax
import jax.numpy as jnp
from jax import lax
from jax.experimental import pallas as pl
from jax.experimental.pallas import tpu as pltpu
from jax.sharding import PartitionSpec as P


residual_scale = 8.0**0.25
norm_eps = 1e-05
LANES = 128
F32 = jnp.float32


def exchange(pieces, axis, groups=None):
    return lax.all_to_all(
        pieces, axis, split_axis=0, concat_axis=0, tiled=True, axis_index_groups=groups
    )


def after(x, earlier):
    return lax.optimization_barrier((x, earlier))[0]


def step_of(held, bit):
    size = lax.axis_size("dp")
    return lax.ppermute(held, "dp", [(i, i ^ bit) for i in range(size)])


def merged(held, got):
    return lax.optimization_barrier(jnp.concatenate([held, got]))


def chain_order(size):
    held, bit = [0], size // 2
    while bit > 1:
        held = held + [h ^ bit for h in held]
        bit //= 2
    return held


def row_dot(x, turned):
    return lax.dot_general(x, turned, (((1,), (1,)), ((), ())), preferred_element_type=F32)


class Weights:
    def __init__(self, low, high, order, whole, held_ref, got_ref, buffer_ref, sems):
        self.order, self.whole, self.buffer = order, whole, buffer_ref
        self.copies = [
            pltpu.make_async_copy(ref.at[:, low:high, :], buffer_ref.at[half], sems.at[half])
            for half, ref in enumerate((held_ref, got_ref))
        ]
        for copy in self.copies:
            copy.start()

    def dot(self, x_ref):
        me = lax.axis_index("dp")
        base = me if self.whole else me & 1
        rows = self.buffer.shape[3]
        total = jnp.zeros((x_ref.shape[-2], self.buffer.shape[2]), F32)
        for half, copy in enumerate(self.copies):
            copy.wait()
            for slot, other in enumerate(self.order):
                at = base ^ (other ^ half)
                if len(x_ref.shape) == 3:
                    total = total + row_dot(x_ref[at], self.buffer[half, slot])
                else:
                    at = pl.multiple_of(at * rows, rows)
                    total = total + row_dot(x_ref[:, pl.ds(at, rows)], self.buffer[half, slot])
        return total


def weight_space(held, columns):
    shape = (2, held.shape[0], columns, held.shape[2])
    return [pltpu.VMEM(shape, held.dtype), pltpu.SemaphoreType.DMA((2,))]


def pair_up(pieces_ref, width, at):
    two = [pieces_ref[2 * at + k][:, :width].astype(F32) for k in range(2)]
    return jnp.concatenate(two, axis=1)


def spread(ref, x):
    if x.shape[1] < LANES:
        x = jnp.concatenate([x, jnp.zeros((x.shape[0], LANES - x.shape[1]), x.dtype)], axis=1)
    x = x.astype(ref.dtype)
    for copy in range(ref.shape[0]):
        ref[copy] = x


def call(kernel, out_shape, *arrays, flops=10**6, scratch=(), specs=None, out_specs=None, aliases=None):
    moved = sum(a.size * a.dtype.itemsize for a in arrays)
    extra = {} if specs is None else {"in_specs": specs}
    if out_specs is not None:
        extra["grid"] = (1,)
    if out_specs is not None:
        extra["out_specs"] = out_specs
    return pl.pallas_call(
        kernel,
        out_shape=out_shape,
        scratch_shapes=list(scratch),
        input_output_aliases=aliases or {},
        cost_estimate=pl.CostEstimate(flops=flops, bytes_accessed=moved, transcendentals=0),
        compiler_params=pltpu.CompilerParams(vmem_limit_bytes=32 * 2**20),
        **extra,
    )(*arrays)


def one_block(shape, at=None):
    at = at or (0,) * len(shape)
    return pl.BlockSpec(shape, lambda step: at)


def first_kernel(cut, fetch, pieces_ref, held_ref, got_ref, x_ref, qk_ref, vo_ref, *space):
    weights = Weights(*fetch, held_ref, got_ref, *space)
    width = x_ref.shape[1] // pieces_ref.shape[0]
    for at in range(pieces_ref.shape[0] // 2):
        cols = slice(2 * width * at, 2 * width * (at + 1))
        x_ref[:, cols] = pair_up(pieces_ref, width, at).astype(x_ref.dtype)
    out = weights.dot(x_ref)
    spread(qk_ref, out[:, :cut])
    vo_ref[...] = out[:, cut:].astype(vo_ref.dtype)


def norm_kernel(cut, fetch, pieces_ref, gain_ref, held_ref, got_ref, x_ref, qk_ref, vo_ref, *space):
    weights = Weights(*fetch, held_ref, got_ref, *space)
    count, width = pieces_ref.shape[0], x_ref.shape[1] // pieces_ref.shape[0]
    pairs = [pair_up(pieces_ref, width, at) for at in range(count // 2)]
    features = x_ref.shape[1]
    mean = jnp.sum(sum(pairs), axis=1, keepdims=True) / features
    pairs = [p - mean for p in pairs]
    variance = jnp.sum(sum(p * p for p in pairs), axis=1, keepdims=True) / features
    scale = lax.rsqrt(variance + norm_eps)
    for at, p in enumerate(pairs):
        cols = slice(2 * width * at, 2 * width * (at + 1))
        x_ref[:, cols] = (p * scale * gain_ref[:, cols]).astype(x_ref.dtype)
    out = weights.dot(x_ref)
    spread(qk_ref, out[:, :cut])
    vo_ref[...] = out[:, cut:].astype(vo_ref.dtype)


def head_sums(x, heads):
    x = x.reshape(heads, -1, *x.shape[1:]).sum(1)
    lane = lax.broadcasted_iota(jnp.int32, (x.shape[1], LANES), 1)
    sums = jnp.sum(x, axis=2, keepdims=True)
    total = jnp.zeros((x.shape[1], LANES), F32)
    for head in range(heads):
        total = jnp.where(lane == head, sums[head], total)
    return total


def side_pairs(x):
    return jnp.stack([jnp.concatenate([x[at], x[at + 1]], axis=1) for at in range(0, len(x), 2)])


def readout_kernel(scale, pieces_ref, vo_ref, retain_ref, admit_ref, state_ref, normalizer_ref, out_ref):
    heads = retain_ref.shape[1]
    width = vo_ref.shape[1] // 2
    both = pieces_ref[...].astype(F32)
    query = side_pairs(both[:, :, :width])
    key = side_pairs(both[:, :, width : 2 * width]) * scale
    retain, admit = retain_ref[...], admit_ref[...]
    of_key = head_sums(query * key, heads)[:, :heads] * admit
    of_normalizer = head_sums(query * normalizer_ref[...], heads)[:, :heads] * retain
    divisor = jnp.maximum(jnp.abs(of_normalizer + of_key), 1.0)
    vo = vo_ref[...].astype(F32)
    parts = []
    for e in range(state_ref.shape[0]):
        numerator = head_sums(query * state_ref[e], heads)[:, :heads] * retain
        value = vo[:, e * heads : (e + 1) * heads]
        gate = vo[:, width + e * heads : width + (e + 1) * heads]
        parts.append((numerator + value * of_key) / divisor * jax.nn.sigmoid(gate))
    spread(out_ref, jnp.concatenate(parts, axis=1))


def branch_kernel(width, fetch, pieces_ref, x_ref, held_ref, got_ref, out_ref, wide_ref, *space):
    weights = Weights(*fetch, held_ref, got_ref, *space)
    blocks, seqs, rows = wide_ref.shape
    count = pieces_ref.shape[0] // blocks
    for at in range(blocks):
        found = [pieces_ref[count * at + k][:, :width].astype(F32) for k in range(count)]
        found.append(jnp.zeros((seqs, rows - count * width), F32))
        wide_ref[at] = jnp.concatenate(found, axis=1).astype(wide_ref.dtype)
    branch = weights.dot(wide_ref)
    spread(out_ref, residual_scale * x_ref[...].astype(F32) + branch)


def last_kernel(features, pieces_ref, gain_ref, out_ref):
    width = out_ref.shape[1]
    pieces = [pieces_ref[at].astype(F32) for at in range(pieces_ref.shape[0])]
    mean = jnp.sum(sum(pieces), axis=1, keepdims=True) / features
    lane = lax.broadcasted_iota(jnp.int32, pieces[0].shape, 1)
    off = [jnp.where(lane < width, p - mean, 0.0) for p in pieces]
    variance = jnp.sum(sum(p * p for p in off), axis=1, keepdims=True) / features
    own = pieces_ref[lax.axis_index("tp")].astype(F32)[:, :width]
    out = (own - mean) * lax.rsqrt(variance + norm_eps) * gain_ref[...]
    out_ref[...] = out.astype(out_ref.dtype)


def column(row, heads):
    at = lax.broadcasted_iota(jnp.int32, (heads, heads), 0)
    lane = lax.broadcasted_iota(jnp.int32, (heads, heads), 1)
    wide = jnp.broadcast_to(row, (heads, heads))
    return jnp.sum(jnp.where(at == lane, wide, 0.0), axis=1, keepdims=True)


def update_kernel(scale, parts, *refs):
    pieces_ref, vo_ref, retain_ref, admit_ref, state_ref, normalizer_ref = refs[:6]
    new_state_ref, new_normalizer_ref, rows_ref = refs[-3:]
    _, seqs, channels, heads, size = state_ref.shape
    width = size // parts
    rows_ref[...] = pieces_ref[...].astype(F32).reshape(rows_ref.shape)
    vo = vo_ref[...].astype(F32)
    for seq in range(seqs):
        found = [
            rows_ref[pl.ds(seq + seqs * part, heads, stride=seqs * parts), :]
            for part in range(parts)
        ]
        key = jnp.concatenate([f[:, width : 2 * width] for f in found], axis=1) * scale
        retain = column(retain_ref[seq : seq + 1, :], heads)
        admit = column(admit_ref[seq : seq + 1, :], heads)
        new_normalizer_ref[0, seq] = retain * normalizer_ref[0, seq] + admit * key
        for e in range(channels):
            value = column(vo[seq : seq + 1, e * heads : (e + 1) * heads], heads)
            new_state_ref[0, seq, e] = retain * state_ref[0, seq, e] + (admit * value) * key


def update(block_no, saved, state, normalizer, made):
    size, width = state.shape[4], saved[1].shape[1] // 2
    blocks = [
        one_block((1, *x.shape[1:]), (block_no,) + (0,) * (x.ndim - 1)) for x in (state, normalizer)
    ]
    whole = [one_block(x.shape) for x in saved]
    arrays = (*saved, state, normalizer, *made)
    return call(
        functools.partial(update_kernel, size**-0.5, size // width),
        [jax.ShapeDtypeStruct(x.shape, x.dtype) for x in (state, normalizer)],
        *arrays,
        scratch=[pltpu.VMEM((saved[0].shape[0] * saved[0].shape[1], LANES), F32)],
        specs=[*whole, *blocks, *[pl.BlockSpec(memory_space=pl.ANY) for _ in made]],
        out_specs=blocks,
        aliases={6: 0, 7: 1} if made else None,
    )


def shards(
    stream,
    query_weight,
    key_weight,
    value_weight,
    outgate_weight,
    gate_weight,
    gate_bias,
    output_weight,
    norm_gain,
    matrix_state,
    normalizer_state,
    stabilizer_state,
):
    head_count = gate_bias.shape[1] // 2
    head_size = normalizer_state.shape[3]
    seqs, feats = stream.shape
    rows, cols = query_weight.shape[1:]
    peers = lax.axis_size("tp")
    owners = lax.axis_size("dp")
    order = chain_order(owners)
    by_chip = [2 * chip for chip in range(owners // 2)]
    me = lax.axis_index("tp")
    bf16 = stream.dtype
    copies = jax.ShapeDtypeStruct((peers, seqs, LANES), bf16)
    pair = jax.ShapeDtypeStruct((seqs, 2 * cols), bf16)
    pair_cols = 2 * cols
    per_head = head_size // pair_cols
    turned = [jnp.swapaxes(w, 1, 2) for w in (query_weight, key_weight, value_weight, outgate_weight)]
    out_turned = jnp.swapaxes(output_weight, 1, 2)
    short = ((0, 0), (0, rows - out_turned.shape[2]))

    bulk = jnp.concatenate([w[0] for w in turned] + [jnp.pad(out_turned[0], short)])
    later = after((turned, out_turned), bulk)
    chain = jnp.concatenate([w[1] for w in later[0]] + [jnp.pad(later[1][1], short)])[None]
    held_in = pl.BlockSpec(memory_space=pltpu.MemorySpace.HBM)
    here = pl.BlockSpec(memory_space=pltpu.MemorySpace.VMEM)

    def by_piece(x):
        x = x.reshape(*x.shape[:-1], per_head, pair_cols)
        return jnp.moveaxis(x, 0, -2).reshape(*x.shape[1:-3], peers // 2, seqs, pair_cols)

    states = [by_piece(m) for m in matrix_state]
    normalizers = [by_piece(n) for n in normalizer_state]

    chips = [[2 * chip + core for chip in range(owners // 2)] for core in range(2)]
    bulk = jnp.broadcast_to(bulk, (owners // 2, *bulk.shape))
    bulk = exchange(bulk, "dp", chips)
    tile = jnp.pad(stream, ((0, 0), (0, LANES - feats)))
    tile = after(tile, (*states, *normalizers, bulk))
    pieces = exchange(jnp.broadcast_to(tile, copies.shape), "tp")
    got_bulk = step_of(bulk, 1)
    got = step_of(chain, 8)
    x_local = stream
    whole_x = jax.ShapeDtypeStruct((seqs, peers * feats), bf16)
    saved, new_stabs = ([], [])
    for block_no in range(gate_bias.shape[0]):
        if block_no == 0:
            halves = (bulk, got_bulk)
            fetch = (by_chip, False)
            x_full, qk, vo = call(
                functools.partial(first_kernel, 2 * cols, (0, 4 * cols, *fetch)),
                (whole_x, copies, pair),
                pieces,
                *halves,
                specs=[here, held_in, held_in],
                scratch=weight_space(bulk, 4 * cols),
            )
            chain = merged(after(chain, (qk,)), got)
            got = step_of(chain, 4)
        else:
            halves = (chain, got)
            fetch = (order, True)
            x_full, qk, vo = call(
                functools.partial(norm_kernel, 2 * cols, (0, 4 * cols, *fetch)),
                (whole_x, copies, pair),
                pieces,
                norm_gain[:1],
                *halves,
                specs=[here, here, held_in, held_in],
                scratch=weight_space(chain, 4 * cols),
            )
            x_local = lax.dynamic_slice_in_dim(x_full, me * feats, feats, 1)
            tied = after(saved[0], (qk,))
            made = update(0, tied, matrix_state, normalizer_state, ())
        pieces = exchange(qk, "tp")
        gate_pre = (
            jnp.dot(x_full, gate_weight[block_no], preferred_element_type=F32)
            + gate_bias[block_no]
        )
        log_in = gate_pre[:, :head_count]
        log_forget = jax.nn.log_sigmoid(gate_pre[:, head_count:])
        old_stab = stabilizer_state[block_no]
        stab_new = jnp.maximum(log_forget + old_stab, log_in)
        retain = jnp.exp(log_forget + old_stab - stab_new)
        admit = jnp.exp(log_in - stab_new)
        hidden = call(
            functools.partial(readout_kernel, head_size**-0.5),
            copies,
            pieces,
            vo,
            retain,
            admit,
            states[block_no],
            normalizers[block_no],
        )
        if block_no == 0:
            chain = merged(after(chain, (hidden,)), got)
            got = step_of(chain, 2)
        saved.append((pieces, vo, retain, admit))
        pieces = exchange(hidden, "tp")
        summed = call(
            functools.partial(branch_kernel, cols, (4 * cols, 4 * cols + feats, *fetch)),
            copies,
            pieces,
            x_local,
            *halves,
            specs=[here, here, held_in, held_in],
            scratch=[pltpu.VMEM((owners, seqs, rows), bf16), *weight_space(halves[0], feats)],
        )
        if block_no == 0:
            chain = merged(after(chain, (summed,)), got)
            got = step_of(chain, 1)
        new_stabs.append(stab_new)
        pieces = exchange(summed, "tp")
    gain = lax.dynamic_slice_in_dim(norm_gain[1:], me * feats, feats, 1)
    out = call(
        functools.partial(last_kernel, peers * feats),
        jax.ShapeDtypeStruct((seqs, feats), bf16),
        pieces,
        gain,
    )
    made = update(1, after(saved[1], (summed,)), matrix_state, normalizer_state, made)
    return (out, *made, jnp.stack(new_stabs))


def solution(mesh):
    return jax.shard_map(
        shards,
        mesh=mesh,
        in_specs=(
            P("dp", "tp"),
            P(None, "dp", "tp"),
            P(None, "dp", "tp"),
            P(None, "dp", "tp"),
            P(None, "dp", "tp"),
            P(),
            P(),
            P(None, "dp", "tp"),
            P(),
            P(None, "dp", "tp", None, None),
            P(None, "dp", None, None),
            P(None, "dp", None),
        ),
        out_specs=(
            P("dp", "tp"),
            P(None, "dp", "tp", None, None),
            P(None, "dp", None, None),
            P(None, "dp", None),
        ),
        check_vma=False,
    )
```

```python
import functools

import jax
import jax.numpy as jnp
from jax import lax
from jax.experimental import pallas as pl
from jax.experimental.pallas import tpu as pltpu
from jax.sharding import PartitionSpec as P


residual_scale = 8.0**0.25
norm_eps = 1e-05
LANES = 128
F32 = jnp.float32


def exchange(pieces, axis):
    return lax.all_to_all(pieces, axis, split_axis=0, concat_axis=0, tiled=True)


def after(x, earlier):
    return lax.optimization_barrier((x, earlier))[0]


def step_of(held, bit):
    size = lax.axis_size("dp")
    return lax.ppermute(held, "dp", [(i, i ^ bit) for i in range(size)])


def merged(held, got):
    return lax.optimization_barrier(jnp.concatenate([held, got]))


def chain_order(size):
    held, bit = [0], size // 2
    while bit > 1:
        held = held + [h ^ bit for h in held]
        bit //= 2
    return held


def row_dot(x, turned):
    return lax.dot_general(x, turned, (((1,), (1,)), ((), ())), preferred_element_type=F32)


class Weights:
    def __init__(self, low, high, order, whole, held_ref, got_ref, buffer_ref, sems):
        self.order, self.whole, self.buffer = order, whole, buffer_ref
        self.copies = [
            pltpu.make_async_copy(ref.at[:, low:high, :], buffer_ref.at[half], sems.at[half])
            for half, ref in enumerate((held_ref, got_ref))
        ]
        for copy in self.copies:
            copy.start()

    def dot(self, x_ref):
        me = lax.axis_index("dp")
        base = me if self.whole else me & 1
        rows = self.buffer.shape[3]
        total = jnp.zeros((x_ref.shape[-2], self.buffer.shape[2]), F32)
        for half, copy in enumerate(self.copies):
            copy.wait()
            for slot, other in enumerate(self.order):
                at = base ^ (other ^ half)
                if len(x_ref.shape) == 3:
                    total = total + row_dot(x_ref[at], self.buffer[half, slot])
                else:
                    at = pl.multiple_of(at * rows, rows)
                    total = total + row_dot(x_ref[:, pl.ds(at, rows)], self.buffer[half, slot])
        return total


def weight_space(held, columns):
    shape = (2, held.shape[0], columns, held.shape[2])
    return [pltpu.VMEM(shape, held.dtype), pltpu.SemaphoreType.DMA((2,))]


def pair_up(pieces_ref, width, at):
    two = [pieces_ref[2 * at + k][:, :width].astype(F32) for k in range(2)]
    return jnp.concatenate(two, axis=1)


def spread(ref, x):
    if x.shape[1] < LANES:
        x = jnp.concatenate([x, jnp.zeros((x.shape[0], LANES - x.shape[1]), x.dtype)], axis=1)
    x = x.astype(ref.dtype)
    for copy in range(ref.shape[0]):
        ref[copy] = x


def call(kernel, out_shape, *arrays, flops=10**6, scratch=(), specs=None, out_specs=None, aliases=None):
    moved = sum(a.size * a.dtype.itemsize for a in arrays)
    extra = {} if specs is None else {"in_specs": specs}
    if out_specs is not None:
        extra["grid"] = (1,)
    if out_specs is not None:
        extra["out_specs"] = out_specs
    return pl.pallas_call(
        kernel,
        out_shape=out_shape,
        scratch_shapes=list(scratch),
        input_output_aliases=aliases or {},
        cost_estimate=pl.CostEstimate(flops=flops, bytes_accessed=moved, transcendentals=0),
        compiler_params=pltpu.CompilerParams(vmem_limit_bytes=32 * 2**20),
        **extra,
    )(*arrays)


def one_block(shape, at=None):
    at = at or (0,) * len(shape)
    return pl.BlockSpec(shape, lambda step: at)


def pack_kernel(*refs):
    *project_refs, output_ref, own_ref, chain_ref = refs
    at = 0
    for ref in project_refs:
        size = ref.shape[1]
        own_ref[at : at + size, :] = ref[0]
        chain_ref[0, at : at + size, :] = ref[1]
        at += size
    blocks, size, rows = output_ref.shape
    for block in range(blocks):
        chain_ref[0, at : at + size, :rows] = output_ref[block]
        chain_ref[0, at : at + size, rows:] = jnp.zeros(
            (size, chain_ref.shape[2] - rows), chain_ref.dtype
        )
        at += size


def whole_kernel(pieces_ref, x_ref, cut_ref):
    width = x_ref.shape[1] // pieces_ref.shape[0]
    rows = cut_ref.shape[2]
    for at in range(pieces_ref.shape[0] // 2):
        low = 2 * width * at
        pair = pair_up(pieces_ref, width, at).astype(x_ref.dtype)
        x_ref[:, low : low + 2 * width] = pair
        cut_ref[low // rows, :, low % rows : low % rows + 2 * width] = pair


def partial_kernel(x_ref, weight_ref, out_ref):
    owners, seqs, rows = x_ref.shape
    x = x_ref[...].reshape(owners * seqs, rows)
    out = row_dot(x, weight_ref[...])
    out_ref[...] = out.reshape(out_ref.shape).astype(out_ref.dtype)


def sum_kernel(cut, parts_ref, qk_ref, vo_ref):
    out = sum(parts_ref[at].astype(F32) for at in range(parts_ref.shape[0]))
    spread(qk_ref, out[:, :cut])
    vo_ref[...] = out[:, cut:].astype(vo_ref.dtype)


def norm_kernel(cut, fetch, pieces_ref, gain_ref, held_ref, got_ref, x_ref, qk_ref, vo_ref, *space):
    weights = Weights(*fetch, held_ref, got_ref, *space)
    count, width = pieces_ref.shape[0], x_ref.shape[1] // pieces_ref.shape[0]
    pairs = [pair_up(pieces_ref, width, at) for at in range(count // 2)]
    features = x_ref.shape[1]
    mean = jnp.sum(sum(pairs), axis=1, keepdims=True) / features
    pairs = [p - mean for p in pairs]
    variance = jnp.sum(sum(p * p for p in pairs), axis=1, keepdims=True) / features
    scale = lax.rsqrt(variance + norm_eps)
    for at, p in enumerate(pairs):
        cols = slice(2 * width * at, 2 * width * (at + 1))
        x_ref[:, cols] = (p * scale * gain_ref[:, cols]).astype(x_ref.dtype)
    out = weights.dot(x_ref)
    spread(qk_ref, out[:, :cut])
    vo_ref[...] = out[:, cut:].astype(vo_ref.dtype)


def head_sums(x, heads):
    x = x.reshape(heads, -1, *x.shape[1:]).sum(1)
    lane = lax.broadcasted_iota(jnp.int32, (x.shape[1], LANES), 1)
    sums = jnp.sum(x, axis=2, keepdims=True)
    total = jnp.zeros((x.shape[1], LANES), F32)
    for head in range(heads):
        total = jnp.where(lane == head, sums[head], total)
    return total


def side_pairs(x):
    return jnp.stack([jnp.concatenate([x[at], x[at + 1]], axis=1) for at in range(0, len(x), 2)])


def readout_kernel(scale, pieces_ref, vo_ref, retain_ref, admit_ref, state_ref, normalizer_ref, out_ref):
    heads = retain_ref.shape[1]
    width = vo_ref.shape[1] // 2
    both = pieces_ref[...].astype(F32)
    query = side_pairs(both[:, :, :width])
    key = side_pairs(both[:, :, width : 2 * width]) * scale
    retain, admit = retain_ref[...], admit_ref[...]
    of_key = head_sums(query * key, heads)[:, :heads] * admit
    of_normalizer = head_sums(query * normalizer_ref[...], heads)[:, :heads] * retain
    divisor = jnp.maximum(jnp.abs(of_normalizer + of_key), 1.0)
    vo = vo_ref[...].astype(F32)
    parts = []
    for e in range(state_ref.shape[0]):
        numerator = head_sums(query * state_ref[e], heads)[:, :heads] * retain
        value = vo[:, e * heads : (e + 1) * heads]
        gate = vo[:, width + e * heads : width + (e + 1) * heads]
        parts.append((numerator + value * of_key) / divisor * jax.nn.sigmoid(gate))
    spread(out_ref, jnp.concatenate(parts, axis=1))


def branch_kernel(width, fetch, pieces_ref, x_ref, held_ref, got_ref, out_ref, wide_ref, *space):
    weights = Weights(*fetch, held_ref, got_ref, *space)
    blocks, seqs, rows = wide_ref.shape
    count = pieces_ref.shape[0] // blocks
    for at in range(blocks):
        found = [pieces_ref[count * at + k][:, :width].astype(F32) for k in range(count)]
        found.append(jnp.zeros((seqs, rows - count * width), F32))
        wide_ref[at] = jnp.concatenate(found, axis=1).astype(wide_ref.dtype)
    branch = weights.dot(wide_ref)
    spread(out_ref, residual_scale * x_ref[...].astype(F32) + branch)


def last_kernel(features, pieces_ref, gain_ref, out_ref):
    width = out_ref.shape[1]
    pieces = [pieces_ref[at].astype(F32) for at in range(pieces_ref.shape[0])]
    mean = jnp.sum(sum(pieces), axis=1, keepdims=True) / features
    lane = lax.broadcasted_iota(jnp.int32, pieces[0].shape, 1)
    off = [jnp.where(lane < width, p - mean, 0.0) for p in pieces]
    variance = jnp.sum(sum(p * p for p in off), axis=1, keepdims=True) / features
    own = pieces_ref[lax.axis_index("tp")].astype(F32)[:, :width]
    out = (own - mean) * lax.rsqrt(variance + norm_eps) * gain_ref[...]
    out_ref[...] = out.astype(out_ref.dtype)


def column(row, heads):
    at = lax.broadcasted_iota(jnp.int32, (heads, heads), 0)
    lane = lax.broadcasted_iota(jnp.int32, (heads, heads), 1)
    wide = jnp.broadcast_to(row, (heads, heads))
    return jnp.sum(jnp.where(at == lane, wide, 0.0), axis=1, keepdims=True)


def update_kernel(scale, parts, *refs):
    pieces_ref, vo_ref, retain_ref, admit_ref, state_ref, normalizer_ref = refs[:6]
    new_state_ref, new_normalizer_ref, rows_ref = refs[-3:]
    _, seqs, channels, heads, size = state_ref.shape
    width = size // parts
    rows_ref[...] = pieces_ref[...].astype(F32).reshape(rows_ref.shape)
    vo = vo_ref[...].astype(F32)
    for seq in range(seqs):
        found = [
            rows_ref[pl.ds(seq + seqs * part, heads, stride=seqs * parts), :]
            for part in range(parts)
        ]
        key = jnp.concatenate([f[:, width : 2 * width] for f in found], axis=1) * scale
        retain = column(retain_ref[seq : seq + 1, :], heads)
        admit = column(admit_ref[seq : seq + 1, :], heads)
        new_normalizer_ref[0, seq] = retain * normalizer_ref[0, seq] + admit * key
        for e in range(channels):
            value = column(vo[seq : seq + 1, e * heads : (e + 1) * heads], heads)
            new_state_ref[0, seq, e] = retain * state_ref[0, seq, e] + (admit * value) * key


def update(block_no, saved, state, normalizer, made):
    size, width = state.shape[4], saved[1].shape[1] // 2
    blocks = [
        one_block((1, *x.shape[1:]), (block_no,) + (0,) * (x.ndim - 1)) for x in (state, normalizer)
    ]
    whole = [one_block(x.shape) for x in saved]
    arrays = (*saved, state, normalizer, *made)
    return call(
        functools.partial(update_kernel, size**-0.5, size // width),
        [jax.ShapeDtypeStruct(x.shape, x.dtype) for x in (state, normalizer)],
        *arrays,
        scratch=[pltpu.VMEM((saved[0].shape[0] * saved[0].shape[1], LANES), F32)],
        specs=[*whole, *blocks, *[pl.BlockSpec(memory_space=pl.ANY) for _ in made]],
        out_specs=blocks,
        aliases={6: 0, 7: 1} if made else None,
    )


def shards(
    stream,
    query_weight,
    key_weight,
    value_weight,
    outgate_weight,
    gate_weight,
    gate_bias,
    output_weight,
    norm_gain,
    matrix_state,
    normalizer_state,
    stabilizer_state,
):
    head_count = gate_bias.shape[1] // 2
    head_size = normalizer_state.shape[3]
    seqs, feats = stream.shape
    rows, cols = query_weight.shape[1:]
    peers = lax.axis_size("tp")
    owners = lax.axis_size("dp")
    order = chain_order(owners)
    me = lax.axis_index("tp")
    bf16 = stream.dtype
    copies = jax.ShapeDtypeStruct((peers, seqs, LANES), bf16)
    pair = jax.ShapeDtypeStruct((seqs, 2 * cols), bf16)
    pair_cols = 2 * cols
    per_head = head_size // pair_cols
    turned = [jnp.swapaxes(w, 1, 2) for w in (query_weight, key_weight, value_weight, outgate_weight)]
    out_turned = jnp.swapaxes(output_weight, 1, 2)
    held_in = pl.BlockSpec(memory_space=pltpu.MemorySpace.HBM)
    here = pl.BlockSpec(memory_space=pltpu.MemorySpace.VMEM)
    own, chain = call(
        pack_kernel,
        (
            jax.ShapeDtypeStruct((4 * cols, rows), bf16),
            jax.ShapeDtypeStruct((1, 4 * cols + 2 * feats, rows), bf16),
        ),
        *turned,
        out_turned,
    )

    def by_piece(x):
        x = x.reshape(*x.shape[:-1], per_head, pair_cols)
        return jnp.moveaxis(x, 0, -2).reshape(*x.shape[1:-3], peers // 2, seqs, pair_cols)

    states = [by_piece(m) for m in matrix_state]
    normalizers = [by_piece(n) for n in normalizer_state]

    whole_x = jax.ShapeDtypeStruct((seqs, peers * feats), bf16)
    tile = jnp.pad(stream, ((0, 0), (0, LANES - feats)))
    pieces = exchange(jnp.broadcast_to(tile, copies.shape), "tp")
    got = step_of(chain, 8)
    x_local = stream
    x_full, cut = call(
        whole_kernel, (whole_x, jax.ShapeDtypeStruct((owners, seqs, rows), bf16)), pieces
    )
    everyone = exchange(cut, "dp")
    partial = call(
        partial_kernel, jax.ShapeDtypeStruct((owners, seqs, 4 * cols), bf16), everyone, own
    )
    partial = after(partial, (states, normalizers))
    parts = exchange(partial, "dp")
    chain = merged(after(chain, (partial,)), got)
    got = step_of(chain, 4)
    saved, new_stabs = ([], [])
    for block_no in range(gate_bias.shape[0]):
        if block_no == 0:
            qk, vo = call(functools.partial(sum_kernel, 2 * cols), (copies, pair), parts)
            chain = merged(after(chain, (qk,)), got)
            got = step_of(chain, 2)
        else:
            x_full, qk, vo = call(
                functools.partial(norm_kernel, 2 * cols, (0, 4 * cols, order, True)),
                (whole_x, copies, pair),
                pieces,
                norm_gain[:1],
                chain,
                got,
                specs=[here, here, held_in, held_in],
                scratch=weight_space(chain, 4 * cols),
            )
            x_local = lax.dynamic_slice_in_dim(x_full, me * feats, feats, 1)
            tied = after(saved[0], (qk,))
            made = update(0, tied, matrix_state, normalizer_state, ())
        pieces = exchange(qk, "tp")
        gate_pre = (
            jnp.dot(x_full, gate_weight[block_no], preferred_element_type=F32)
            + gate_bias[block_no]
        )
        log_in = gate_pre[:, :head_count]
        log_forget = jax.nn.log_sigmoid(gate_pre[:, head_count:])
        old_stab = stabilizer_state[block_no]
        stab_new = jnp.maximum(log_forget + old_stab, log_in)
        retain = jnp.exp(log_forget + old_stab - stab_new)
        admit = jnp.exp(log_in - stab_new)
        hidden = call(
            functools.partial(readout_kernel, head_size**-0.5),
            copies,
            pieces,
            vo,
            retain,
            admit,
            states[block_no],
            normalizers[block_no],
        )
        if block_no == 0:
            chain = merged(after(chain, (hidden,)), got)
            got = step_of(chain, 1)
        saved.append((pieces, vo, retain, admit))
        pieces = exchange(hidden, "tp")
        low = 4 * cols + block_no * feats
        summed = call(
            functools.partial(branch_kernel, cols, (low, low + feats, order, True)),
            copies,
            pieces,
            x_local,
            chain,
            got,
            specs=[here, here, held_in, held_in],
            scratch=[pltpu.VMEM((owners, seqs, rows), bf16), *weight_space(chain, feats)],
        )
        new_stabs.append(stab_new)
        pieces = exchange(summed, "tp")
    gain = lax.dynamic_slice_in_dim(norm_gain[1:], me * feats, feats, 1)
    out = call(
        functools.partial(last_kernel, peers * feats),
        jax.ShapeDtypeStruct((seqs, feats), bf16),
        pieces,
        gain,
    )
    made = update(1, after(saved[1], (summed,)), matrix_state, normalizer_state, made)
    return (out, *made, jnp.stack(new_stabs))


def solution(mesh):
    return jax.shard_map(
        shards,
        mesh=mesh,
        in_specs=(
            P("dp", "tp"),
            P(None, "dp", "tp"),
            P(None, "dp", "tp"),
            P(None, "dp", "tp"),
            P(None, "dp", "tp"),
            P(),
            P(),
            P(None, "dp", "tp"),
            P(),
            P(None, "dp", "tp", None, None),
            P(None, "dp", None, None),
            P(None, "dp", None),
        ),
        out_specs=(
            P("dp", "tp"),
            P(None, "dp", "tp", None, None),
            P(None, "dp", None, None),
            P(None, "dp", None),
        ),
        check_vma=False,
    )
```

```python
import functools

import jax
import jax.numpy as jnp
from jax import lax
from jax.experimental import pallas as pl
from jax.experimental.pallas import tpu as pltpu
from jax.sharding import PartitionSpec as P


residual_scale = 8.0**0.25
norm_eps = 1e-05
LANES = 128
F32 = jnp.float32


def exchange(pieces, axis):
    return lax.all_to_all(pieces, axis, split_axis=0, concat_axis=0, tiled=True)


def after(x, earlier):
    return lax.optimization_barrier((x, earlier))[0]


def to_chip(x, away):
    size = lax.axis_size("dp")
    return lax.ppermute(x, "dp", [(i, (i + 2 * away) % size) for i in range(size)])


def to_other_core(x):
    size = lax.axis_size("dp")
    return lax.ppermute(x, "dp", [(i, i ^ 1) for i in range(size)])


def row_dot(x, turned):
    return lax.dot_general(x, turned, (((1,), (1,)), ((), ())), preferred_element_type=F32)


def blocks_dot(x_ref, halves, places, low=0, high=None):
    me = lax.axis_index("dp")
    owners = 2 * len(places)
    rows = halves[0].shape[2]
    total = None
    for half, ref in enumerate(halves):
        for slot, away in enumerate(places):
            at = lax.rem(me + (2 * away + owners), owners) ^ half
            if len(x_ref.shape) == 3:
                x = x_ref[at]
            else:
                x = x_ref[:, pl.ds(pl.multiple_of(at * rows, rows), rows)]
            product = row_dot(x, ref[slot, low:high, :])
            total = product if total is None else total + product
    return total


def pair_up(pieces_ref, width, at):
    two = [pieces_ref[2 * at + k][:, :width].astype(F32) for k in range(2)]
    return jnp.concatenate(two, axis=1)


def spread(ref, x):
    if x.shape[1] < LANES:
        x = jnp.concatenate([x, jnp.zeros((x.shape[0], LANES - x.shape[1]), x.dtype)], axis=1)
    x = x.astype(ref.dtype)
    for copy in range(ref.shape[0]):
        ref[copy] = x


def call(kernel, out_shape, *arrays, flops=10**6, scratch=(), specs=None, out_specs=None, aliases=None):
    moved = sum(a.size * a.dtype.itemsize for a in arrays)
    extra = {} if specs is None else {"in_specs": specs}
    if out_specs is not None:
        extra["grid"] = (1,)
    if out_specs is not None:
        extra["out_specs"] = out_specs
    return pl.pallas_call(
        kernel,
        out_shape=out_shape,
        scratch_shapes=list(scratch),
        input_output_aliases=aliases or {},
        cost_estimate=pl.CostEstimate(flops=flops, bytes_accessed=moved, transcendentals=0),
        compiler_params=pltpu.CompilerParams(vmem_limit_bytes=32 * 2**20),
        **extra,
    )(*arrays)


def one_block(shape, at=None):
    at = at or (0,) * len(shape)
    return pl.BlockSpec(shape, lambda step: at)


def pack_kernel(*refs):
    count = (len(refs) - 3) // 2
    given, (own_ref, ring_ref), found, sems = refs[:count], refs[count : count + 2], refs[count + 2 : -1], refs[-1]
    fetches = [pltpu.make_async_copy(g, f, sems.at[k]) for k, (g, f) in enumerate(zip(given, found))]
    for fetch in fetches:
        fetch.start()
    for fetch in fetches:
        fetch.wait()
    *projections, output = found
    at = 0
    for ref in projections:
        size = ref.shape[1]
        own_ref[at : at + size, :] = ref[0]
        ring_ref[at : at + size, :] = ref[1]
        at += size
    blocks, size, rows = output.shape
    for block in range(blocks):
        ring_ref[at : at + size, :rows] = output[block]
        ring_ref[at : at + size, rows:] = jnp.zeros((size, ring_ref.shape[1] - rows), ring_ref.dtype)
        at += size


def stack_kernel(*refs):
    for at, ref in enumerate(refs[:-1]):
        refs[-1][at] = ref[...]


def whole_kernel(pieces_ref, x_ref, cut_ref):
    width = x_ref.shape[1] // pieces_ref.shape[0]
    rows = cut_ref.shape[2]
    for at in range(pieces_ref.shape[0] // 2):
        low = 2 * width * at
        pair = pair_up(pieces_ref, width, at).astype(x_ref.dtype)
        x_ref[:, low : low + 2 * width] = pair
        cut_ref[low // rows, :, low % rows : low % rows + 2 * width] = pair


def partial_kernel(x_ref, weight_ref, out_ref):
    owners, seqs, rows = x_ref.shape
    x = x_ref[...].reshape(owners * seqs, rows)
    out = row_dot(x, weight_ref[...])
    out_ref[...] = out.reshape(out_ref.shape).astype(out_ref.dtype)


def sum_kernel(cut, parts_ref, qk_ref, vo_ref):
    out = sum(parts_ref[at].astype(F32) for at in range(parts_ref.shape[0]))
    spread(qk_ref, out[:, :cut])
    vo_ref[...] = out[:, cut:].astype(vo_ref.dtype)


def norm_kernel(cut, high, places, pieces_ref, gain_ref, held_ref, got_ref, x_ref, qk_ref, vo_ref):
    count, width = pieces_ref.shape[0], x_ref.shape[1] // pieces_ref.shape[0]
    pairs = [pair_up(pieces_ref, width, at) for at in range(count // 2)]
    features = x_ref.shape[1]
    mean = jnp.sum(sum(pairs), axis=1, keepdims=True) / features
    pairs = [p - mean for p in pairs]
    variance = jnp.sum(sum(p * p for p in pairs), axis=1, keepdims=True) / features
    scale = lax.rsqrt(variance + norm_eps)
    for at, p in enumerate(pairs):
        cols = slice(2 * width * at, 2 * width * (at + 1))
        x_ref[:, cols] = (p * scale * gain_ref[:, cols]).astype(x_ref.dtype)
    out = blocks_dot(x_ref, (held_ref, got_ref), places, 0, high)
    spread(qk_ref, out[:, :cut])
    vo_ref[...] = out[:, cut:].astype(vo_ref.dtype)


def head_sums(x, heads):
    x = x.reshape(heads, -1, *x.shape[1:]).sum(1)
    lane = lax.broadcasted_iota(jnp.int32, (x.shape[1], LANES), 1)
    sums = jnp.sum(x, axis=2, keepdims=True)
    total = jnp.zeros((x.shape[1], LANES), F32)
    for head in range(heads):
        total = jnp.where(lane == head, sums[head], total)
    return total


def side_pairs(x):
    return jnp.stack([jnp.concatenate([x[at], x[at + 1]], axis=1) for at in range(0, len(x), 2)])


def readout_kernel(scale, pieces_ref, vo_ref, retain_ref, admit_ref, state_ref, normalizer_ref, out_ref):
    heads = retain_ref.shape[1]
    width = vo_ref.shape[1] // 2
    both = pieces_ref[...].astype(F32)
    query = side_pairs(both[:, :, :width])
    key = side_pairs(both[:, :, width : 2 * width]) * scale
    retain, admit = retain_ref[...], admit_ref[...]
    of_key = head_sums(query * key, heads)[:, :heads] * admit
    of_normalizer = head_sums(query * normalizer_ref[...], heads)[:, :heads] * retain
    divisor = jnp.maximum(jnp.abs(of_normalizer + of_key), 1.0)
    vo = vo_ref[...].astype(F32)
    parts = []
    for e in range(state_ref.shape[0]):
        numerator = head_sums(query * state_ref[e], heads)[:, :heads] * retain
        value = vo[:, e * heads : (e + 1) * heads]
        gate = vo[:, width + e * heads : width + (e + 1) * heads]
        parts.append((numerator + value * of_key) / divisor * jax.nn.sigmoid(gate))
    spread(out_ref, jnp.concatenate(parts, axis=1))


def branch_kernel(width, low, high, places, pieces_ref, x_ref, held_ref, got_ref, out_ref, wide_ref):
    blocks, seqs, rows = wide_ref.shape
    count = pieces_ref.shape[0] // blocks
    for at in range(blocks):
        found = [pieces_ref[count * at + k][:, :width].astype(F32) for k in range(count)]
        found.append(jnp.zeros((seqs, rows - count * width), F32))
        wide_ref[at] = jnp.concatenate(found, axis=1).astype(wide_ref.dtype)
    branch = blocks_dot(wide_ref, (held_ref, got_ref), places, low, high)
    spread(out_ref, residual_scale * x_ref[...].astype(F32) + branch)


def last_kernel(features, pieces_ref, gain_ref, out_ref):
    width = out_ref.shape[1]
    pieces = [pieces_ref[at].astype(F32) for at in range(pieces_ref.shape[0])]
    mean = jnp.sum(sum(pieces), axis=1, keepdims=True) / features
    lane = lax.broadcasted_iota(jnp.int32, pieces[0].shape, 1)
    off = [jnp.where(lane < width, p - mean, 0.0) for p in pieces]
    variance = jnp.sum(sum(p * p for p in off), axis=1, keepdims=True) / features
    own = pieces_ref[lax.axis_index("tp")].astype(F32)[:, :width]
    out = (own - mean) * lax.rsqrt(variance + norm_eps) * gain_ref[...]
    out_ref[...] = out.astype(out_ref.dtype)


def column(row, heads):
    at = lax.broadcasted_iota(jnp.int32, (heads, heads), 0)
    lane = lax.broadcasted_iota(jnp.int32, (heads, heads), 1)
    wide = jnp.broadcast_to(row, (heads, heads))
    return jnp.sum(jnp.where(at == lane, wide, 0.0), axis=1, keepdims=True)


def update_kernel(scale, parts, *refs):
    pieces_ref, vo_ref, retain_ref, admit_ref, state_ref, normalizer_ref = refs[:6]
    new_state_ref, new_normalizer_ref, rows_ref = refs[-3:]
    _, seqs, channels, heads, size = state_ref.shape
    width = size // parts
    rows_ref[...] = pieces_ref[...].astype(F32).reshape(rows_ref.shape)
    vo = vo_ref[...].astype(F32)
    for seq in range(seqs):
        found = [
            rows_ref[pl.ds(seq + seqs * part, heads, stride=seqs * parts), :]
            for part in range(parts)
        ]
        key = jnp.concatenate([f[:, width : 2 * width] for f in found], axis=1) * scale
        retain = column(retain_ref[seq : seq + 1, :], heads)
        admit = column(admit_ref[seq : seq + 1, :], heads)
        new_normalizer_ref[0, seq] = retain * normalizer_ref[0, seq] + admit * key
        for e in range(channels):
            value = column(vo[seq : seq + 1, e * heads : (e + 1) * heads], heads)
            new_state_ref[0, seq, e] = retain * state_ref[0, seq, e] + (admit * value) * key


def update(block_no, saved, state, normalizer, made):
    size, width = state.shape[4], saved[1].shape[1] // 2
    blocks = [
        one_block((1, *x.shape[1:]), (block_no,) + (0,) * (x.ndim - 1)) for x in (state, normalizer)
    ]
    whole = [one_block(x.shape) for x in saved]
    arrays = (*saved, state, normalizer, *made)
    return call(
        functools.partial(update_kernel, size**-0.5, size // width),
        [jax.ShapeDtypeStruct(x.shape, x.dtype) for x in (state, normalizer)],
        *arrays,
        scratch=[pltpu.VMEM((saved[0].shape[0] * saved[0].shape[1], LANES), F32)],
        specs=[*whole, *blocks, *[pl.BlockSpec(memory_space=pl.ANY) for _ in made]],
        out_specs=blocks,
        aliases={6: 0, 7: 1} if made else None,
    )


def shards(
    stream,
    query_weight,
    key_weight,
    value_weight,
    outgate_weight,
    gate_weight,
    gate_bias,
    output_weight,
    norm_gain,
    matrix_state,
    normalizer_state,
    stabilizer_state,
):
    head_count = gate_bias.shape[1] // 2
    head_size = normalizer_state.shape[3]
    seqs, feats = stream.shape
    rows, cols = query_weight.shape[1:]
    peers = lax.axis_size("tp")
    owners = lax.axis_size("dp")
    places = (0, -1, 1, -2, 2, -3, 3, -4)
    assert owners == 2 * len(places)
    me = lax.axis_index("tp")
    bf16 = stream.dtype
    copies = jax.ShapeDtypeStruct((peers, seqs, LANES), bf16)
    pair = jax.ShapeDtypeStruct((seqs, 2 * cols), bf16)
    pair_cols = 2 * cols
    per_head = head_size // pair_cols
    turned = [jnp.swapaxes(w, 1, 2) for w in (query_weight, key_weight, value_weight, outgate_weight)]
    out_turned = jnp.swapaxes(output_weight, 1, 2)
    held_in = pl.BlockSpec(memory_space=pltpu.MemorySpace.HBM)
    given = (*turned, out_turned)
    own, ring = call(
        pack_kernel,
        (
            jax.ShapeDtypeStruct((4 * cols, rows), bf16),
            jax.ShapeDtypeStruct((4 * cols + 2 * feats, rows), bf16),
        ),
        *given,
        specs=[held_in] * len(given),
        scratch=[*[pltpu.VMEM(w.shape, bf16) for w in given], pltpu.SemaphoreType.DMA((len(given),))],
    )

    def by_piece(x):
        x = x.reshape(*x.shape[:-1], per_head, pair_cols)
        return jnp.moveaxis(x, 0, -2).reshape(*x.shape[1:-3], peers // 2, seqs, pair_cols)

    states = [by_piece(m) for m in matrix_state]
    normalizers = [by_piece(n) for n in normalizer_state]

    whole_x = jax.ShapeDtypeStruct((seqs, peers * feats), bf16)
    tile = jnp.pad(stream, ((0, 0), (0, LANES - feats)))
    pieces = exchange(jnp.broadcast_to(tile, copies.shape), "tp")
    right, left = [to_chip(ring, 1)], [to_chip(ring, -1)]
    x_local = stream
    x_full, cut = call(
        whole_kernel, (whole_x, jax.ShapeDtypeStruct((owners, seqs, rows), bf16)), pieces
    )
    everyone = exchange(cut, "dp")
    right.append(to_chip(right[-1], 1))
    left.append(to_chip(left[-1], -1))
    partial = call(
        partial_kernel, jax.ShapeDtypeStruct((owners, seqs, 4 * cols), bf16), everyone, own
    )
    partial = after(partial, (states, normalizers))
    parts = exchange(partial, "dp")
    right.append(to_chip(right[-1], 1))
    left.append(to_chip(left[-1], -1))
    saved, new_stabs = ([], [])
    for block_no in range(gate_bias.shape[0]):
        if block_no == 0:
            qk, vo = call(functools.partial(sum_kernel, 2 * cols), (copies, pair), parts)
            right.append(to_chip(right[-1], 1))
        else:
            x_full, qk, vo = call(
                functools.partial(norm_kernel, 2 * cols, 4 * cols, places),
                (whole_x, copies, pair),
                pieces,
                norm_gain[:1],
                *halves,
            )
            halves = after(halves, qk)
            halves = [h[:, 4 * cols + feats :] for h in halves]
            x_local = lax.dynamic_slice_in_dim(x_full, me * feats, feats, 1)
            tied = after(saved[0], (qk,))
            made = update(0, tied, matrix_state, normalizer_state, ())
        pieces = exchange(qk, "tp")
        gate_pre = (
            jnp.dot(x_full, gate_weight[block_no], preferred_element_type=F32)
            + gate_bias[block_no]
        )
        log_in = gate_pre[:, :head_count]
        log_forget = jax.nn.log_sigmoid(gate_pre[:, head_count:])
        old_stab = stabilizer_state[block_no]
        stab_new = jnp.maximum(log_forget + old_stab, log_in)
        retain = jnp.exp(log_forget + old_stab - stab_new)
        admit = jnp.exp(log_in - stab_new)
        hidden = call(
            functools.partial(readout_kernel, head_size**-0.5),
            copies,
            pieces,
            vo,
            retain,
            admit,
            states[block_no],
            normalizers[block_no],
        )
        if block_no == 0:
            blocks = [ring]
            for place in range(4):
                blocks += [right[place], *left[place : place + 1]]
            held = call(
                stack_kernel,
                jax.ShapeDtypeStruct((len(blocks), *ring.shape), bf16),
                *after(blocks, hidden),
            )
            halves = (held, to_other_core(held))
        saved.append((pieces, vo, retain, admit))
        pieces = exchange(hidden, "tp")
        low = 4 * cols * (1 - block_no)
        summed = call(
            functools.partial(branch_kernel, cols, low, low + feats, places),
            copies,
            pieces,
            x_local,
            *halves,
            scratch=[pltpu.VMEM((owners, seqs, rows), bf16)],
        )
        new_stabs.append(stab_new)
        pieces = exchange(summed, "tp")
    gain = lax.dynamic_slice_in_dim(norm_gain[1:], me * feats, feats, 1)
    out = call(
        functools.partial(last_kernel, peers * feats),
        jax.ShapeDtypeStruct((seqs, feats), bf16),
        pieces,
        gain,
    )
    made = update(1, after(saved[1], (summed,)), matrix_state, normalizer_state, made)
    return (out, *made, jnp.stack(new_stabs))


def solution(mesh):
    return jax.shard_map(
        shards,
        mesh=mesh,
        in_specs=(
            P("dp", "tp"),
            P(None, "dp", "tp"),
            P(None, "dp", "tp"),
            P(None, "dp", "tp"),
            P(None, "dp", "tp"),
            P(),
            P(),
            P(None, "dp", "tp"),
            P(),
            P(None, "dp", "tp", None, None),
            P(None, "dp", None, None),
            P(None, "dp", None),
        ),
        out_specs=(
            P("dp", "tp"),
            P(None, "dp", "tp", None, None),
            P(None, "dp", None, None),
            P(None, "dp", None),
        ),
        check_vma=False,
    )
```

```python
import functools

import jax
import jax.numpy as jnp
from jax import lax
from jax.experimental import pallas as pl
from jax.experimental.pallas import tpu as pltpu
from jax.sharding import PartitionSpec as P


residual_scale = 8.0**0.25
norm_eps = 1e-05
LANES = 128
MOST_VMEM = 67_043_328
F32 = jnp.float32


def exchange(pieces, axis):
    return lax.all_to_all(pieces, axis, split_axis=0, concat_axis=0, tiled=True)


def after(x, earlier):
    return lax.optimization_barrier((x, earlier))[0]


def step_of(held, bit):
    size = lax.axis_size("dp")
    return lax.ppermute(held, "dp", [(i, i ^ bit) for i in range(size)])


def merged(held, got):
    return lax.optimization_barrier(jnp.concatenate([held, got]))


def chain_order(size):
    held, bit = [0], size // 2
    while bit > 1:
        held = held + [h ^ bit for h in held]
        bit //= 2
    return held


def row_dot(x, turned):
    return lax.dot_general(x, turned, (((1,), (1,)), ((), ())), preferred_element_type=F32)


def blocks_dot(x_ref, halves, order, low=0, high=None):
    me = lax.axis_index("dp")
    rows = halves[0].shape[2]
    total = None
    for half, ref in enumerate(halves):
        for slot, other in enumerate(order):
            at = me ^ (other ^ half)
            if len(x_ref.shape) == 3:
                x = x_ref[at]
            else:
                x = x_ref[:, pl.ds(pl.multiple_of(at * rows, rows), rows)]
            product = row_dot(x, ref[slot, low:high, :])
            total = product if total is None else total + product
    return total


def pair_up(pieces_ref, width, at):
    two = [pieces_ref[2 * at + k][:, :width].astype(F32) for k in range(2)]
    return jnp.concatenate(two, axis=1)


def spread(ref, x):
    if x.shape[1] < LANES:
        x = jnp.concatenate([x, jnp.zeros((x.shape[0], LANES - x.shape[1]), x.dtype)], axis=1)
    x = x.astype(ref.dtype)
    for copy in range(ref.shape[0]):
        ref[copy] = x


def call(kernel, out_shape, *arrays, flops=10**6, scratch=(), specs=None, out_specs=None, aliases=None, room=32 * 2**20):
    moved = sum(a.size * a.dtype.itemsize for a in arrays)
    extra = {} if specs is None else {"in_specs": specs}
    if out_specs is not None:
        extra["grid"] = (1,)
    if out_specs is not None:
        extra["out_specs"] = out_specs
    return pl.pallas_call(
        kernel,
        out_shape=out_shape,
        scratch_shapes=list(scratch),
        input_output_aliases=aliases or {},
        cost_estimate=pl.CostEstimate(flops=flops, bytes_accessed=moved, transcendentals=0),
        compiler_params=pltpu.CompilerParams(vmem_limit_bytes=room),
        **extra,
    )(*arrays)


def one_block(shape, at=None):
    at = at or (0,) * len(shape)
    return pl.BlockSpec(shape, lambda step: at)


def pack_kernel(*refs):
    count = (len(refs) - 3) // 2
    given, (own_ref, chain_ref) = refs[:count], refs[count : count + 2]
    found, sems = refs[count + 2 : -1], refs[-1]
    fetches = [pltpu.make_async_copy(g, f, sems.at[k]) for k, (g, f) in enumerate(zip(given, found))]
    for fetch in fetches:
        fetch.start()
    for fetch in fetches:
        fetch.wait()
    *projections, output = found
    at = 0
    for ref in projections:
        size = ref.shape[1]
        own_ref[at : at + size, :] = ref[0]
        chain_ref[0, at : at + size, :] = ref[1]
        at += size
    blocks, size, rows = output.shape
    for block in range(blocks):
        chain_ref[0, at : at + size, :rows] = output[block]
        chain_ref[0, at : at + size, rows:] = jnp.zeros(
            (size, chain_ref.shape[2] - rows), chain_ref.dtype
        )
        at += size


def copies_kernel(x_ref, out_ref):
    spread(out_ref, x_ref[...].astype(F32))


def whole_kernel(pieces_ref, x_ref, cut_ref):
    width = x_ref.shape[1] // pieces_ref.shape[0]
    rows = cut_ref.shape[2]
    for at in range(pieces_ref.shape[0] // 2):
        low = 2 * width * at
        pair = pair_up(pieces_ref, width, at).astype(x_ref.dtype)
        x_ref[:, low : low + 2 * width] = pair
        cut_ref[low // rows, :, low % rows : low % rows + 2 * width] = pair


def partial_kernel(x_ref, weight_ref, out_ref):
    owners, seqs, rows = x_ref.shape
    x = x_ref[...].reshape(owners * seqs, rows)
    out = row_dot(x, weight_ref[...])
    out_ref[...] = out.reshape(out_ref.shape).astype(out_ref.dtype)


def sum_kernel(cut, parts_ref, qk_ref, vo_ref):
    out = sum(parts_ref[at].astype(F32) for at in range(parts_ref.shape[0]))
    spread(qk_ref, out[:, :cut])
    vo_ref[...] = out[:, cut:].astype(vo_ref.dtype)


def norm_kernel(cut, high, order, pieces_ref, gain_ref, held_ref, got_ref, x_ref, qk_ref, vo_ref):
    count, width = pieces_ref.shape[0], x_ref.shape[1] // pieces_ref.shape[0]
    pairs = [pair_up(pieces_ref, width, at) for at in range(count // 2)]
    features = x_ref.shape[1]
    mean = jnp.sum(sum(pairs), axis=1, keepdims=True) / features
    pairs = [p - mean for p in pairs]
    variance = jnp.sum(sum(p * p for p in pairs), axis=1, keepdims=True) / features
    scale = lax.rsqrt(variance + norm_eps)
    for at, p in enumerate(pairs):
        cols = slice(2 * width * at, 2 * width * (at + 1))
        x_ref[:, cols] = (p * scale * gain_ref[:, cols]).astype(x_ref.dtype)
    out = blocks_dot(x_ref, (held_ref, got_ref), order, 0, high)
    spread(qk_ref, out[:, :cut])
    vo_ref[...] = out[:, cut:].astype(vo_ref.dtype)


def head_sums(x, heads):
    x = x.reshape(heads, -1, *x.shape[1:]).sum(1)
    lane = lax.broadcasted_iota(jnp.int32, (x.shape[1], LANES), 1)
    sums = jnp.sum(x, axis=2, keepdims=True)
    total = jnp.zeros((x.shape[1], LANES), F32)
    for head in range(heads):
        total = jnp.where(lane == head, sums[head], total)
    return total


def side_pairs(x):
    return jnp.stack([jnp.concatenate([x[at], x[at + 1]], axis=1) for at in range(0, len(x), 2)])


def readout_kernel(scale, pieces_ref, vo_ref, retain_ref, admit_ref, state_ref, normalizer_ref, out_ref):
    heads = retain_ref.shape[1]
    width = vo_ref.shape[1] // 2
    both = pieces_ref[...].astype(F32)
    query = side_pairs(both[:, :, :width])
    key = side_pairs(both[:, :, width : 2 * width]) * scale
    retain, admit = retain_ref[...], admit_ref[...]
    of_key = head_sums(query * key, heads)[:, :heads] * admit
    of_normalizer = head_sums(query * normalizer_ref[...], heads)[:, :heads] * retain
    divisor = jnp.maximum(jnp.abs(of_normalizer + of_key), 1.0)
    vo = vo_ref[...].astype(F32)
    parts = []
    for e in range(state_ref.shape[0]):
        numerator = head_sums(query * state_ref[e], heads)[:, :heads] * retain
        value = vo[:, e * heads : (e + 1) * heads]
        gate = vo[:, width + e * heads : width + (e + 1) * heads]
        parts.append((numerator + value * of_key) / divisor * jax.nn.sigmoid(gate))
    spread(out_ref, jnp.concatenate(parts, axis=1))


def branch_kernel(width, low, high, order, pieces_ref, x_ref, held_ref, got_ref, out_ref, wide_ref):
    blocks, seqs, rows = wide_ref.shape
    count = pieces_ref.shape[0] // blocks
    for at in range(blocks):
        found = [pieces_ref[count * at + k][:, :width].astype(F32) for k in range(count)]
        found.append(jnp.zeros((seqs, rows - count * width), F32))
        wide_ref[at] = jnp.concatenate(found, axis=1).astype(wide_ref.dtype)
    branch = blocks_dot(wide_ref, (held_ref, got_ref), order, low, high)
    spread(out_ref, residual_scale * x_ref[...].astype(F32) + branch)


def last_kernel(features, pieces_ref, gain_ref, out_ref):
    width = out_ref.shape[1]
    pieces = [pieces_ref[at].astype(F32) for at in range(pieces_ref.shape[0])]
    mean = jnp.sum(sum(pieces), axis=1, keepdims=True) / features
    lane = lax.broadcasted_iota(jnp.int32, pieces[0].shape, 1)
    off = [jnp.where(lane < width, p - mean, 0.0) for p in pieces]
    variance = jnp.sum(sum(p * p for p in off), axis=1, keepdims=True) / features
    own = pieces_ref[lax.axis_index("tp")].astype(F32)[:, :width]
    out = (own - mean) * lax.rsqrt(variance + norm_eps) * gain_ref[...]
    out_ref[...] = out.astype(out_ref.dtype)


def column(row, heads):
    at = lax.broadcasted_iota(jnp.int32, (heads, heads), 0)
    lane = lax.broadcasted_iota(jnp.int32, (heads, heads), 1)
    wide = jnp.broadcast_to(row, (heads, heads))
    return jnp.sum(jnp.where(at == lane, wide, 0.0), axis=1, keepdims=True)


def update_kernel(scale, parts, *refs):
    pieces_ref, vo_ref, retain_ref, admit_ref, state_ref, normalizer_ref = refs[:6]
    new_state_ref, new_normalizer_ref, rows_ref = refs[-3:]
    _, seqs, channels, heads, size = state_ref.shape
    width = size // parts
    rows_ref[...] = pieces_ref[...].astype(F32).reshape(rows_ref.shape)
    vo = vo_ref[...].astype(F32)
    for seq in range(seqs):
        found = [
            rows_ref[pl.ds(seq + seqs * part, heads, stride=seqs * parts), :]
            for part in range(parts)
        ]
        key = jnp.concatenate([f[:, width : 2 * width] for f in found], axis=1) * scale
        retain = column(retain_ref[seq : seq + 1, :], heads)
        admit = column(admit_ref[seq : seq + 1, :], heads)
        new_normalizer_ref[0, seq] = retain * normalizer_ref[0, seq] + admit * key
        for e in range(channels):
            value = column(vo[seq : seq + 1, e * heads : (e + 1) * heads], heads)
            new_state_ref[0, seq, e] = retain * state_ref[0, seq, e] + (admit * value) * key


def update(block_no, saved, state, normalizer, made):
    size, width = state.shape[4], saved[1].shape[1] // 2
    blocks = [
        one_block((1, *x.shape[1:]), (block_no,) + (0,) * (x.ndim - 1)) for x in (state, normalizer)
    ]
    whole = [one_block(x.shape) for x in saved]
    arrays = (*saved, state, normalizer, *made)
    return call(
        functools.partial(update_kernel, size**-0.5, size // width),
        [jax.ShapeDtypeStruct(x.shape, x.dtype) for x in (state, normalizer)],
        *arrays,
        scratch=[pltpu.VMEM((saved[0].shape[0] * saved[0].shape[1], LANES), F32)],
        specs=[*whole, *blocks, *[pl.BlockSpec(memory_space=pl.ANY) for _ in made]],
        out_specs=blocks,
        aliases={6: 0, 7: 1} if made else None,
        room=MOST_VMEM - 400 * 2**10,
    )


def shards(
    stream,
    query_weight,
    key_weight,
    value_weight,
    outgate_weight,
    gate_weight,
    gate_bias,
    output_weight,
    norm_gain,
    matrix_state,
    normalizer_state,
    stabilizer_state,
):
    head_count = gate_bias.shape[1] // 2
    head_size = normalizer_state.shape[3]
    seqs, feats = stream.shape
    rows, cols = query_weight.shape[1:]
    peers = lax.axis_size("tp")
    owners = lax.axis_size("dp")
    order = chain_order(owners)
    me = lax.axis_index("tp")
    bf16 = stream.dtype
    copies = jax.ShapeDtypeStruct((peers, seqs, LANES), bf16)
    pair = jax.ShapeDtypeStruct((seqs, 2 * cols), bf16)
    pair_cols = 2 * cols
    per_head = head_size // pair_cols
    turned = [jnp.swapaxes(w, 1, 2) for w in (query_weight, key_weight, value_weight, outgate_weight)]
    out_turned = jnp.swapaxes(output_weight, 1, 2)
    held_in = pl.BlockSpec(memory_space=pltpu.MemorySpace.HBM)
    given = (*turned, out_turned)
    own, chain = call(
        pack_kernel,
        (
            jax.ShapeDtypeStruct((4 * cols, rows), bf16),
            jax.ShapeDtypeStruct((1, 4 * cols + 2 * feats, rows), bf16),
        ),
        *given,
        specs=[held_in] * len(given),
        scratch=[*[pltpu.VMEM(w.shape, bf16) for w in given], pltpu.SemaphoreType.DMA((len(given),))],
        room=MOST_VMEM - 160 * 2**10,
    )

    def by_piece(x):
        x = x.reshape(*x.shape[:-1], per_head, pair_cols)
        return jnp.moveaxis(x, 0, -2).reshape(*x.shape[1:-3], peers // 2, seqs, pair_cols)

    whole_x = jax.ShapeDtypeStruct((seqs, peers * feats), bf16)
    pieces = exchange(call(copies_kernel, copies, stream), "tp")
    got = step_of(chain, 8)
    x_local = stream
    x_full, cut = call(
        whole_kernel, (whole_x, jax.ShapeDtypeStruct((owners, seqs, rows), bf16)), pieces
    )
    seen = after((matrix_state, normalizer_state), cut)
    states = [by_piece(m) for m in seen[0]]
    normalizers = [by_piece(n) for n in seen[1]]
    everyone = exchange(cut, "dp")
    partial = call(
        partial_kernel, jax.ShapeDtypeStruct((owners, seqs, 4 * cols), bf16), everyone, own
    )
    partial = after(partial, (states, normalizers))
    parts = exchange(partial, "dp")
    chain = merged(after(chain, (partial,)), got)
    got = step_of(chain, 4)
    saved, new_stabs = ([], [])
    for block_no in range(gate_bias.shape[0]):
        if block_no == 0:
            qk, vo = call(functools.partial(sum_kernel, 2 * cols), (copies, pair), parts)
            chain = merged(after(chain, (qk,)), got)
            got = step_of(chain, 2)
        else:
            x_full, qk, vo = call(
                functools.partial(norm_kernel, 2 * cols, 4 * cols, order),
                (whole_x, copies, pair),
                pieces,
                norm_gain[:1],
                chain,
                got,
            )
            x_local = lax.dynamic_slice_in_dim(x_full, me * feats, feats, 1)
            tied = after(saved[0], (qk,))
            made = update(0, tied, matrix_state, normalizer_state, ())
        pieces = exchange(qk, "tp")
        gate_pre = (
            jnp.dot(x_full, gate_weight[block_no], preferred_element_type=F32)
            + gate_bias[block_no]
        )
        log_in = gate_pre[:, :head_count]
        log_forget = jax.nn.log_sigmoid(gate_pre[:, head_count:])
        old_stab = stabilizer_state[block_no]
        stab_new = jnp.maximum(log_forget + old_stab, log_in)
        retain = jnp.exp(log_forget + old_stab - stab_new)
        admit = jnp.exp(log_in - stab_new)
        hidden = call(
            functools.partial(readout_kernel, head_size**-0.5),
            copies,
            pieces,
            vo,
            retain,
            admit,
            states[block_no],
            normalizers[block_no],
        )
        if block_no == 0:
            chain = merged(after(chain, (hidden,)), got)
            got = step_of(chain, 1)
        saved.append((pieces, vo, retain, admit))
        pieces = exchange(hidden, "tp")
        low = 4 * cols + block_no * feats
        summed = call(
            functools.partial(branch_kernel, cols, low, low + feats, order),
            copies,
            pieces,
            x_local,
            chain,
            got,
            scratch=[pltpu.VMEM((owners, seqs, rows), bf16)],
        )
        new_stabs.append(stab_new)
        pieces = exchange(summed, "tp")
    gain = lax.dynamic_slice_in_dim(norm_gain[1:], me * feats, feats, 1)
    out = call(
        functools.partial(last_kernel, peers * feats),
        jax.ShapeDtypeStruct((seqs, feats), bf16),
        pieces,
        gain,
    )
    made = update(1, after(saved[1], (summed,)), matrix_state, normalizer_state, made)
    return (out, *made, jnp.stack(new_stabs))


def solution(mesh):
    return jax.shard_map(
        shards,
        mesh=mesh,
        in_specs=(
            P("dp", "tp"),
            P(None, "dp", "tp"),
            P(None, "dp", "tp"),
            P(None, "dp", "tp"),
            P(None, "dp", "tp"),
            P(),
            P(),
            P(None, "dp", "tp"),
            P(),
            P(None, "dp", "tp", None, None),
            P(None, "dp", None, None),
            P(None, "dp", None),
        ),
        out_specs=(
            P("dp", "tp"),
            P(None, "dp", "tp", None, None),
            P(None, "dp", None, None),
            P(None, "dp", None),
        ),
        check_vma=False,
    )
```

```python
import functools

import jax
import jax.numpy as jnp
from jax import lax
from jax.experimental import pallas as pl
from jax.experimental.pallas import tpu as pltpu
from jax.sharding import PartitionSpec as P


residual_scale = 8.0**0.25
norm_eps = 1e-05
LANES = 128
MOST_VMEM = 67_043_328
F32 = jnp.float32


def exchange(pieces, axis):
    return lax.all_to_all(pieces, axis, split_axis=0, concat_axis=0, tiled=True)


def after(x, earlier):
    return lax.optimization_barrier((x, earlier))[0]


def step_of(held, bit):
    size = lax.axis_size("dp")
    return lax.ppermute(held, "dp", [(i, i ^ bit) for i in range(size)])


def merged(held, got):
    return lax.optimization_barrier(jnp.concatenate([held, got]))


def chain_order(size):
    held, bit = [0], size // 2
    while bit > 1:
        held = held + [h ^ bit for h in held]
        bit //= 2
    return held


def row_dot(x, turned):
    return lax.dot_general(x, turned, (((1,), (1,)), ((), ())), preferred_element_type=F32)


def blocks_dot(x_ref, halves, order, low=0, high=None):
    me = lax.axis_index("dp")
    rows = halves[0].shape[2]
    total = None
    for half, ref in enumerate(halves):
        for slot, other in enumerate(order):
            at = me ^ (other ^ half)
            if len(x_ref.shape) == 3:
                x = x_ref[at]
            else:
                x = x_ref[:, pl.ds(pl.multiple_of(at * rows, rows), rows)]
            product = row_dot(x, ref[slot, low:high, :])
            total = product if total is None else total + product
    return total


def pair_up(pieces_ref, width, at):
    two = [pieces_ref[2 * at + k][:, :width].astype(F32) for k in range(2)]
    return jnp.concatenate(two, axis=1)


def spread(ref, x):
    if x.shape[1] < LANES:
        x = jnp.concatenate([x, jnp.zeros((x.shape[0], LANES - x.shape[1]), x.dtype)], axis=1)
    x = x.astype(ref.dtype)
    for copy in range(ref.shape[0]):
        ref[copy] = x


def call(kernel, out_shape, *arrays, flops=10**6, scratch=(), specs=None, out_specs=None, aliases=None, room=32 * 2**20):
    moved = sum(a.size * a.dtype.itemsize for a in arrays)
    extra = {} if specs is None else {"in_specs": specs}
    if out_specs is not None:
        extra["grid"] = (1,)
    if out_specs is not None:
        extra["out_specs"] = out_specs
    return pl.pallas_call(
        kernel,
        out_shape=out_shape,
        scratch_shapes=list(scratch),
        input_output_aliases=aliases or {},
        cost_estimate=pl.CostEstimate(flops=flops, bytes_accessed=moved, transcendentals=0),
        compiler_params=pltpu.CompilerParams(vmem_limit_bytes=room),
        **extra,
    )(*arrays)


def one_block(shape, at=None):
    at = at or (0,) * len(shape)
    return pl.BlockSpec(shape, lambda step: at)


def pack_kernel(*refs):
    count = (len(refs) - 3) // 2
    given, (own_ref, chain_ref) = refs[:count], refs[count : count + 2]
    found, sems = refs[count + 2 : -1], refs[-1]
    fetches = [pltpu.make_async_copy(g, f, sems.at[k]) for k, (g, f) in enumerate(zip(given, found))]
    for fetch in fetches:
        fetch.start()
    for fetch in fetches:
        fetch.wait()
    *projections, output = found
    at = 0
    for ref in projections:
        size = ref.shape[1]
        own_ref[at : at + size, :] = ref[0]
        chain_ref[0, at : at + size, :] = ref[1]
        at += size
    blocks, size, rows = output.shape
    for block in range(blocks):
        chain_ref[0, at : at + size, :rows] = output[block]
        chain_ref[0, at : at + size, rows:] = jnp.zeros(
            (size, chain_ref.shape[2] - rows), chain_ref.dtype
        )
        at += size


def copies_kernel(x_ref, out_ref):
    spread(out_ref, x_ref[...].astype(F32))


def whole_kernel(pieces_ref, x_ref, cut_ref):
    width = x_ref.shape[1] // pieces_ref.shape[0]
    rows = cut_ref.shape[2]
    for at in range(pieces_ref.shape[0] // 2):
        low = 2 * width * at
        pair = pair_up(pieces_ref, width, at).astype(x_ref.dtype)
        x_ref[:, low : low + 2 * width] = pair
        cut_ref[low // rows, :, low % rows : low % rows + 2 * width] = pair


def partial_kernel(x_ref, weight_ref, out_ref):
    owners, seqs, rows = x_ref.shape
    x = x_ref[...].reshape(owners * seqs, rows)
    out = row_dot(x, weight_ref[...])
    out_ref[...] = out.reshape(out_ref.shape).astype(out_ref.dtype)


def sum_kernel(cut, parts_ref, qk_ref, vo_ref):
    out = sum(parts_ref[at].astype(F32) for at in range(parts_ref.shape[0]))
    spread(qk_ref, out[:, :cut])
    vo_ref[...] = out[:, cut:].astype(vo_ref.dtype)


def norm_kernel(cut, high, order, pieces_ref, gain_ref, held_ref, got_ref, x_ref, qk_ref, vo_ref):
    count, width = pieces_ref.shape[0], x_ref.shape[1] // pieces_ref.shape[0]
    pairs = [pair_up(pieces_ref, width, at) for at in range(count // 2)]
    features = x_ref.shape[1]
    mean = jnp.sum(sum(pairs), axis=1, keepdims=True) / features
    pairs = [p - mean for p in pairs]
    variance = jnp.sum(sum(p * p for p in pairs), axis=1, keepdims=True) / features
    scale = lax.rsqrt(variance + norm_eps)
    for at, p in enumerate(pairs):
        cols = slice(2 * width * at, 2 * width * (at + 1))
        x_ref[:, cols] = (p * scale * gain_ref[:, cols]).astype(x_ref.dtype)
    out = blocks_dot(x_ref, (held_ref, got_ref), order, 0, high)
    spread(qk_ref, out[:, :cut])
    vo_ref[...] = out[:, cut:].astype(vo_ref.dtype)


def head_sums(x, heads):
    x = x.reshape(heads, -1, *x.shape[1:]).sum(1)
    lane = lax.broadcasted_iota(jnp.int32, (x.shape[1], LANES), 1)
    sums = jnp.sum(x, axis=2, keepdims=True)
    total = jnp.zeros((x.shape[1], LANES), F32)
    for head in range(heads):
        total = jnp.where(lane == head, sums[head], total)
    return total


def side_pairs(x):
    return jnp.stack([jnp.concatenate([x[at], x[at + 1]], axis=1) for at in range(0, len(x), 2)])


def readout_kernel(scale, pieces_ref, vo_ref, retain_ref, admit_ref, state_ref, normalizer_ref, out_ref):
    heads = retain_ref.shape[1]
    width = vo_ref.shape[1] // 2
    both = pieces_ref[...].astype(F32)
    query = side_pairs(both[:, :, :width])
    key = side_pairs(both[:, :, width : 2 * width]) * scale
    retain, admit = retain_ref[...], admit_ref[...]
    of_key = head_sums(query * key, heads)[:, :heads] * admit
    of_normalizer = head_sums(query * normalizer_ref[...], heads)[:, :heads] * retain
    divisor = jnp.maximum(jnp.abs(of_normalizer + of_key), 1.0)
    vo = vo_ref[...].astype(F32)
    parts = []
    for e in range(state_ref.shape[0]):
        numerator = head_sums(query * state_ref[e], heads)[:, :heads] * retain
        value = vo[:, e * heads : (e + 1) * heads]
        gate = vo[:, width + e * heads : width + (e + 1) * heads]
        parts.append((numerator + value * of_key) / divisor * jax.nn.sigmoid(gate))
    spread(out_ref, jnp.concatenate(parts, axis=1))


def branch_kernel(width, low, high, order, pieces_ref, x_ref, held_ref, got_ref, out_ref, wide_ref):
    blocks, seqs, rows = wide_ref.shape
    count = pieces_ref.shape[0] // blocks
    for at in range(blocks):
        found = [pieces_ref[count * at + k][:, :width].astype(F32) for k in range(count)]
        found.append(jnp.zeros((seqs, rows - count * width), F32))
        wide_ref[at] = jnp.concatenate(found, axis=1).astype(wide_ref.dtype)
    branch = blocks_dot(wide_ref, (held_ref, got_ref), order, low, high)
    spread(out_ref, residual_scale * x_ref[...].astype(F32) + branch)


def last_kernel(features, pieces_ref, gain_ref, out_ref):
    width = out_ref.shape[1]
    pieces = [pieces_ref[at].astype(F32) for at in range(pieces_ref.shape[0])]
    mean = jnp.sum(sum(pieces), axis=1, keepdims=True) / features
    lane = lax.broadcasted_iota(jnp.int32, pieces[0].shape, 1)
    off = [jnp.where(lane < width, p - mean, 0.0) for p in pieces]
    variance = jnp.sum(sum(p * p for p in off), axis=1, keepdims=True) / features
    own = pieces_ref[lax.axis_index("tp")].astype(F32)[:, :width]
    out = (own - mean) * lax.rsqrt(variance + norm_eps) * gain_ref[...]
    out_ref[...] = out.astype(out_ref.dtype)


def column(row, heads):
    at = lax.broadcasted_iota(jnp.int32, (heads, heads), 0)
    lane = lax.broadcasted_iota(jnp.int32, (heads, heads), 1)
    wide = jnp.broadcast_to(row, (heads, heads))
    return jnp.sum(jnp.where(at == lane, wide, 0.0), axis=1, keepdims=True)


def update_kernel(scale, parts, *refs):
    pieces_ref, vo_ref, retain_ref, admit_ref, state_ref, normalizer_ref = refs[:6]
    new_state_ref, new_normalizer_ref, rows_ref = refs[-3:]
    _, seqs, channels, heads, size = state_ref.shape
    width = size // parts
    rows_ref[...] = pieces_ref[...].astype(F32).reshape(rows_ref.shape)
    vo = vo_ref[...].astype(F32)
    for seq in range(seqs):
        found = [
            rows_ref[pl.ds(seq + seqs * part, heads, stride=seqs * parts), :]
            for part in range(parts)
        ]
        key = jnp.concatenate([f[:, width : 2 * width] for f in found], axis=1) * scale
        retain = column(retain_ref[seq : seq + 1, :], heads)
        admit = column(admit_ref[seq : seq + 1, :], heads)
        new_normalizer_ref[0, seq] = retain * normalizer_ref[0, seq] + admit * key
        for e in range(channels):
            value = column(vo[seq : seq + 1, e * heads : (e + 1) * heads], heads)
            new_state_ref[0, seq, e] = retain * state_ref[0, seq, e] + (admit * value) * key


def update(block_no, saved, state, normalizer, made):
    size, width = state.shape[4], saved[1].shape[1] // 2
    blocks = [
        one_block((1, *x.shape[1:]), (block_no,) + (0,) * (x.ndim - 1)) for x in (state, normalizer)
    ]
    whole = [one_block(x.shape) for x in saved]
    arrays = (*saved, state, normalizer, *made)
    return call(
        functools.partial(update_kernel, size**-0.5, size // width),
        [jax.ShapeDtypeStruct(x.shape, x.dtype) for x in (state, normalizer)],
        *arrays,
        scratch=[pltpu.VMEM((saved[0].shape[0] * saved[0].shape[1], LANES), F32)],
        specs=[*whole, *blocks, *[pl.BlockSpec(memory_space=pl.ANY) for _ in made]],
        out_specs=blocks,
        aliases={6: 0, 7: 1} if made else None,
        room=(MOST_VMEM - 400 * 2**10) if made else 60 * 1024 * 2**10,
    )


def shards(
    stream,
    query_weight,
    key_weight,
    value_weight,
    outgate_weight,
    gate_weight,
    gate_bias,
    output_weight,
    norm_gain,
    matrix_state,
    normalizer_state,
    stabilizer_state,
):
    head_count = gate_bias.shape[1] // 2
    head_size = normalizer_state.shape[3]
    seqs, feats = stream.shape
    rows, cols = query_weight.shape[1:]
    peers = lax.axis_size("tp")
    owners = lax.axis_size("dp")
    order = chain_order(owners)
    me = lax.axis_index("tp")
    bf16 = stream.dtype
    copies = jax.ShapeDtypeStruct((peers, seqs, LANES), bf16)
    pair = jax.ShapeDtypeStruct((seqs, 2 * cols), bf16)
    pair_cols = 2 * cols
    per_head = head_size // pair_cols
    turned = [jnp.swapaxes(w, 1, 2) for w in (query_weight, key_weight, value_weight, outgate_weight)]
    out_turned = jnp.swapaxes(output_weight, 1, 2)
    held_in = pl.BlockSpec(memory_space=pltpu.MemorySpace.HBM)
    given = (*turned, out_turned)
    own, chain = call(
        pack_kernel,
        (
            jax.ShapeDtypeStruct((4 * cols, rows), bf16),
            jax.ShapeDtypeStruct((1, 4 * cols + 2 * feats, rows), bf16),
        ),
        *given,
        specs=[held_in] * len(given),
        scratch=[*[pltpu.VMEM(w.shape, bf16) for w in given], pltpu.SemaphoreType.DMA((len(given),))],
        room=MOST_VMEM - 160 * 2**10,
    )

    def by_piece(x):
        x = x.reshape(*x.shape[:-1], per_head, pair_cols)
        return jnp.moveaxis(x, 0, -2).reshape(*x.shape[1:-3], peers // 2, seqs, pair_cols)

    whole_x = jax.ShapeDtypeStruct((seqs, peers * feats), bf16)
    pieces = exchange(call(copies_kernel, copies, stream), "tp")
    got = step_of(chain, 8)
    x_local = stream
    x_full, cut = call(
        whole_kernel, (whole_x, jax.ShapeDtypeStruct((owners, seqs, rows), bf16)), pieces
    )
    seen = after((matrix_state, normalizer_state), cut)
    states = [by_piece(m) for m in seen[0]]
    normalizers = [by_piece(n) for n in seen[1]]
    everyone = exchange(cut, "dp")
    partial = call(
        partial_kernel, jax.ShapeDtypeStruct((owners, seqs, 4 * cols), bf16), everyone, own
    )
    partial = after(partial, (states, normalizers))
    parts = exchange(partial, "dp")
    chain = merged(after(chain, (partial,)), got)
    got = step_of(chain, 4)
    saved, new_stabs = ([], [])
    for block_no in range(gate_bias.shape[0]):
        if block_no == 0:
            qk, vo = call(functools.partial(sum_kernel, 2 * cols), (copies, pair), parts)
            chain = merged(after(chain, (qk,)), got)
            got = step_of(chain, 2)
        else:
            x_full, qk, vo = call(
                functools.partial(norm_kernel, 2 * cols, 4 * cols, order),
                (whole_x, copies, pair),
                pieces,
                norm_gain[:1],
                chain,
                got,
            )
            x_local = lax.dynamic_slice_in_dim(x_full, me * feats, feats, 1)
        pieces = exchange(qk, "tp")
        gate_pre = (
            jnp.dot(x_full, gate_weight[block_no], preferred_element_type=F32)
            + gate_bias[block_no]
        )
        log_in = gate_pre[:, :head_count]
        log_forget = jax.nn.log_sigmoid(gate_pre[:, head_count:])
        old_stab = stabilizer_state[block_no]
        stab_new = jnp.maximum(log_forget + old_stab, log_in)
        retain = jnp.exp(log_forget + old_stab - stab_new)
        admit = jnp.exp(log_in - stab_new)
        hidden = call(
            functools.partial(readout_kernel, head_size**-0.5),
            copies,
            pieces,
            vo,
            retain,
            admit,
            states[block_no],
            normalizers[block_no],
        )
        if block_no == 0:
            chain = merged(after(chain, (hidden,)), got)
            got = step_of(chain, 1)
        saved.append((pieces, vo, retain, admit))
        pieces = exchange(hidden, "tp")
        low = 4 * cols + block_no * feats
        summed = call(
            functools.partial(branch_kernel, cols, low, low + feats, order),
            copies,
            pieces,
            x_local,
            chain,
            got,
            scratch=[pltpu.VMEM((owners, seqs, rows), bf16)],
        )
        if block_no == 0:
            made = update(0, after(saved[0], summed), matrix_state, normalizer_state, ())
        new_stabs.append(stab_new)
        pieces = exchange(summed, "tp")
    gain = lax.dynamic_slice_in_dim(norm_gain[1:], me * feats, feats, 1)
    out = call(
        functools.partial(last_kernel, peers * feats),
        jax.ShapeDtypeStruct((seqs, feats), bf16),
        pieces,
        gain,
    )
    made = update(1, after(saved[1], (summed,)), matrix_state, normalizer_state, made)
    return (out, *made, jnp.stack(new_stabs))


def solution(mesh):
    return jax.shard_map(
        shards,
        mesh=mesh,
        in_specs=(
            P("dp", "tp"),
            P(None, "dp", "tp"),
            P(None, "dp", "tp"),
            P(None, "dp", "tp"),
            P(None, "dp", "tp"),
            P(),
            P(),
            P(None, "dp", "tp"),
            P(),
            P(None, "dp", "tp", None, None),
            P(None, "dp", None, None),
            P(None, "dp", None),
        ),
        out_specs=(
            P("dp", "tp"),
            P(None, "dp", "tp", None, None),
            P(None, "dp", None, None),
            P(None, "dp", None),
        ),
        check_vma=False,
    )
```

```python
import functools

import jax
import jax.numpy as jnp
from jax import lax
from jax.experimental import pallas as pl
from jax.experimental.pallas import tpu as pltpu
from jax.sharding import PartitionSpec as P


residual_scale = 8.0**0.25
norm_eps = 1e-05
LANES = 128
MOST_VMEM = 67_043_328
F32 = jnp.float32


def exchange(pieces, axis):
    return lax.all_to_all(pieces, axis, split_axis=0, concat_axis=0, tiled=True)


def after(x, earlier):
    return lax.optimization_barrier((x, earlier))[0]


def step_of(held, bit):
    size = lax.axis_size("dp")
    return lax.ppermute(held, "dp", [(i, i ^ bit) for i in range(size)])


def merged(held, got):
    return lax.optimization_barrier(jnp.concatenate([held, got]))


def chain_order(size):
    held, bit = [0], size // 2
    while bit > 1:
        held = held + [h ^ bit for h in held]
        bit //= 2
    return held


def row_dot(x, turned):
    return lax.dot_general(x, turned, (((1,), (1,)), ((), ())), preferred_element_type=F32)


def blocks_dot(x_ref, halves, order, low=0, high=None):
    me = lax.axis_index("dp")
    rows = halves[0].shape[2]
    total = None
    for half, ref in enumerate(halves):
        for slot, other in enumerate(order):
            at = me ^ (other ^ half)
            if len(x_ref.shape) == 3:
                x = x_ref[at]
            else:
                x = x_ref[:, pl.ds(pl.multiple_of(at * rows, rows), rows)]
            product = row_dot(x, ref[slot, low:high, :])
            total = product if total is None else total + product
    return total


def pair_up(pieces_ref, width, at):
    two = [pieces_ref[2 * at + k][:, :width].astype(F32) for k in range(2)]
    return jnp.concatenate(two, axis=1)


def spread(ref, x):
    if x.shape[1] < LANES:
        x = jnp.concatenate([x, jnp.zeros((x.shape[0], LANES - x.shape[1]), x.dtype)], axis=1)
    x = x.astype(ref.dtype)
    for copy in range(ref.shape[0]):
        ref[copy] = x


def call(kernel, out_shape, *arrays, flops=10**6, scratch=(), specs=None, out_specs=None, aliases=None, room=32 * 2**20):
    moved = sum(a.size * a.dtype.itemsize for a in arrays)
    extra = {} if specs is None else {"in_specs": specs}
    if out_specs is not None:
        extra["grid"] = (1,)
    if out_specs is not None:
        extra["out_specs"] = out_specs
    return pl.pallas_call(
        kernel,
        out_shape=out_shape,
        scratch_shapes=list(scratch),
        input_output_aliases=aliases or {},
        cost_estimate=pl.CostEstimate(flops=flops, bytes_accessed=moved, transcendentals=0),
        compiler_params=pltpu.CompilerParams(vmem_limit_bytes=room),
        **extra,
    )(*arrays)


def one_block(shape, at=None):
    at = at or (0,) * len(shape)
    return pl.BlockSpec(shape, lambda step: at)


def pack_kernel(*refs):
    count = (len(refs) - 3) // 2
    given, (own_ref, chain_ref) = refs[:count], refs[count : count + 2]
    found, sems = refs[count + 2 : -1], refs[-1]
    fetches = [pltpu.make_async_copy(g, f, sems.at[k]) for k, (g, f) in enumerate(zip(given, found))]
    for fetch in fetches:
        fetch.start()
    for fetch in fetches:
        fetch.wait()
    *projections, output = found
    at = 0
    for ref in projections:
        size = ref.shape[1]
        own_ref[at : at + size, :] = ref[0]
        chain_ref[0, at : at + size, :] = ref[1]
        at += size
    blocks, size, rows = output.shape
    for block in range(blocks):
        chain_ref[0, at : at + size, :rows] = output[block]
        chain_ref[0, at : at + size, rows:] = jnp.zeros(
            (size, chain_ref.shape[2] - rows), chain_ref.dtype
        )
        at += size


def copies_kernel(x_ref, out_ref, here_ref, sem):
    fetch = pltpu.make_async_copy(x_ref, here_ref, sem)
    fetch.start()
    fetch.wait()
    spread(out_ref, here_ref[...].astype(F32))


def whole_kernel(pieces_ref, x_ref, cut_ref):
    width = x_ref.shape[1] // pieces_ref.shape[0]
    rows = cut_ref.shape[2]
    for at in range(pieces_ref.shape[0] // 2):
        low = 2 * width * at
        pair = pair_up(pieces_ref, width, at).astype(x_ref.dtype)
        x_ref[:, low : low + 2 * width] = pair
        cut_ref[low // rows, :, low % rows : low % rows + 2 * width] = pair


def partial_kernel(x_ref, weight_ref, out_ref):
    owners, seqs, rows = x_ref.shape
    x = x_ref[...].reshape(owners * seqs, rows)
    out = row_dot(x, weight_ref[...])
    out_ref[...] = out.reshape(out_ref.shape).astype(out_ref.dtype)


def sum_kernel(cut, parts_ref, qk_ref, vo_ref):
    out = sum(parts_ref[at].astype(F32) for at in range(parts_ref.shape[0]))
    spread(qk_ref, out[:, :cut])
    vo_ref[...] = out[:, cut:].astype(vo_ref.dtype)


def norm_kernel(cut, high, order, pieces_ref, gain_ref, held_ref, got_ref, x_ref, qk_ref, vo_ref):
    count, width = pieces_ref.shape[0], x_ref.shape[1] // pieces_ref.shape[0]
    pairs = [pair_up(pieces_ref, width, at) for at in range(count // 2)]
    features = x_ref.shape[1]
    mean = jnp.sum(sum(pairs), axis=1, keepdims=True) / features
    pairs = [p - mean for p in pairs]
    variance = jnp.sum(sum(p * p for p in pairs), axis=1, keepdims=True) / features
    scale = lax.rsqrt(variance + norm_eps)
    for at, p in enumerate(pairs):
        cols = slice(2 * width * at, 2 * width * (at + 1))
        x_ref[:, cols] = (p * scale * gain_ref[:, cols]).astype(x_ref.dtype)
    out = blocks_dot(x_ref, (held_ref, got_ref), order, 0, high)
    spread(qk_ref, out[:, :cut])
    vo_ref[...] = out[:, cut:].astype(vo_ref.dtype)


def head_sums(x, heads):
    x = x.reshape(heads, -1, *x.shape[1:]).sum(1)
    lane = lax.broadcasted_iota(jnp.int32, (x.shape[1], LANES), 1)
    sums = jnp.sum(x, axis=2, keepdims=True)
    total = jnp.zeros((x.shape[1], LANES), F32)
    for head in range(heads):
        total = jnp.where(lane == head, sums[head], total)
    return total


def side_pairs(x):
    return jnp.stack([jnp.concatenate([x[at], x[at + 1]], axis=1) for at in range(0, len(x), 2)])


def readout_kernel(scale, pieces_ref, vo_ref, retain_ref, admit_ref, state_ref, normalizer_ref, out_ref):
    heads = retain_ref.shape[1]
    width = vo_ref.shape[1] // 2
    both = pieces_ref[...].astype(F32)
    query = side_pairs(both[:, :, :width])
    key = side_pairs(both[:, :, width : 2 * width]) * scale
    retain, admit = retain_ref[...], admit_ref[...]
    of_key = head_sums(query * key, heads)[:, :heads] * admit
    of_normalizer = head_sums(query * normalizer_ref[...], heads)[:, :heads] * retain
    divisor = jnp.maximum(jnp.abs(of_normalizer + of_key), 1.0)
    vo = vo_ref[...].astype(F32)
    parts = []
    for e in range(state_ref.shape[0]):
        numerator = head_sums(query * state_ref[e], heads)[:, :heads] * retain
        value = vo[:, e * heads : (e + 1) * heads]
        gate = vo[:, width + e * heads : width + (e + 1) * heads]
        parts.append((numerator + value * of_key) / divisor * jax.nn.sigmoid(gate))
    spread(out_ref, jnp.concatenate(parts, axis=1))


def branch_kernel(width, low, high, order, pieces_ref, x_ref, held_ref, got_ref, out_ref, wide_ref):
    blocks, seqs, rows = wide_ref.shape
    count = pieces_ref.shape[0] // blocks
    for at in range(blocks):
        found = [pieces_ref[count * at + k][:, :width].astype(F32) for k in range(count)]
        found.append(jnp.zeros((seqs, rows - count * width), F32))
        wide_ref[at] = jnp.concatenate(found, axis=1).astype(wide_ref.dtype)
    branch = blocks_dot(wide_ref, (held_ref, got_ref), order, low, high)
    spread(out_ref, residual_scale * x_ref[...].astype(F32) + branch)


def last_kernel(features, pieces_ref, gain_ref, out_ref):
    width = out_ref.shape[1]
    pieces = [pieces_ref[at].astype(F32) for at in range(pieces_ref.shape[0])]
    mean = jnp.sum(sum(pieces), axis=1, keepdims=True) / features
    lane = lax.broadcasted_iota(jnp.int32, pieces[0].shape, 1)
    off = [jnp.where(lane < width, p - mean, 0.0) for p in pieces]
    variance = jnp.sum(sum(p * p for p in off), axis=1, keepdims=True) / features
    own = pieces_ref[lax.axis_index("tp")].astype(F32)[:, :width]
    out = (own - mean) * lax.rsqrt(variance + norm_eps) * gain_ref[...]
    out_ref[...] = out.astype(out_ref.dtype)


def column(row, heads):
    at = lax.broadcasted_iota(jnp.int32, (heads, heads), 0)
    lane = lax.broadcasted_iota(jnp.int32, (heads, heads), 1)
    wide = jnp.broadcast_to(row, (heads, heads))
    return jnp.sum(jnp.where(at == lane, wide, 0.0), axis=1, keepdims=True)


def update_kernel(scale, parts, *refs):
    pieces_ref, vo_ref, retain_ref, admit_ref, state_ref, normalizer_ref = refs[:6]
    new_state_ref, new_normalizer_ref, rows_ref = refs[-3:]
    _, seqs, channels, heads, size = state_ref.shape
    width = size // parts
    rows_ref[...] = pieces_ref[...].astype(F32).reshape(rows_ref.shape)
    vo = vo_ref[...].astype(F32)
    for seq in range(seqs):
        found = [
            rows_ref[pl.ds(seq + seqs * part, heads, stride=seqs * parts), :]
            for part in range(parts)
        ]
        key = jnp.concatenate([f[:, width : 2 * width] for f in found], axis=1) * scale
        retain = column(retain_ref[seq : seq + 1, :], heads)
        admit = column(admit_ref[seq : seq + 1, :], heads)
        new_normalizer_ref[0, seq] = retain * normalizer_ref[0, seq] + admit * key
        for e in range(channels):
            value = column(vo[seq : seq + 1, e * heads : (e + 1) * heads], heads)
            new_state_ref[0, seq, e] = retain * state_ref[0, seq, e] + (admit * value) * key


def update(block_no, saved, state, normalizer, made):
    size, width = state.shape[4], saved[1].shape[1] // 2
    blocks = [
        one_block((1, *x.shape[1:]), (block_no,) + (0,) * (x.ndim - 1)) for x in (state, normalizer)
    ]
    whole = [one_block(x.shape) for x in saved]
    arrays = (*saved, state, normalizer, *made)
    return call(
        functools.partial(update_kernel, size**-0.5, size // width),
        [jax.ShapeDtypeStruct(x.shape, x.dtype) for x in (state, normalizer)],
        *arrays,
        scratch=[pltpu.VMEM((saved[0].shape[0] * saved[0].shape[1], LANES), F32)],
        specs=[*whole, *blocks, *[pl.BlockSpec(memory_space=pl.ANY) for _ in made]],
        out_specs=blocks,
        aliases={6: 0, 7: 1} if made else None,
        room=(MOST_VMEM - 400 * 2**10) if made else 60 * 1024 * 2**10,
    )


def shards(
    stream,
    query_weight,
    key_weight,
    value_weight,
    outgate_weight,
    gate_weight,
    gate_bias,
    output_weight,
    norm_gain,
    matrix_state,
    normalizer_state,
    stabilizer_state,
):
    head_count = gate_bias.shape[1] // 2
    head_size = normalizer_state.shape[3]
    seqs, feats = stream.shape
    rows, cols = query_weight.shape[1:]
    peers = lax.axis_size("tp")
    owners = lax.axis_size("dp")
    order = chain_order(owners)
    me = lax.axis_index("tp")
    bf16 = stream.dtype
    copies = jax.ShapeDtypeStruct((peers, seqs, LANES), bf16)
    pair = jax.ShapeDtypeStruct((seqs, 2 * cols), bf16)
    pair_cols = 2 * cols
    per_head = head_size // pair_cols
    turned = [jnp.swapaxes(w, 1, 2) for w in (query_weight, key_weight, value_weight, outgate_weight)]
    out_turned = jnp.swapaxes(output_weight, 1, 2)
    held_in = pl.BlockSpec(memory_space=pltpu.MemorySpace.HBM)
    given = (*turned, out_turned)
    own, chain = call(
        pack_kernel,
        (
            jax.ShapeDtypeStruct((4 * cols, rows), bf16),
            jax.ShapeDtypeStruct((1, 4 * cols + 2 * feats, rows), bf16),
        ),
        *given,
        specs=[held_in] * len(given),
        scratch=[*[pltpu.VMEM(w.shape, bf16) for w in given], pltpu.SemaphoreType.DMA((len(given),))],
        room=MOST_VMEM - 160 * 2**10,
    )

    def by_piece(x):
        x = x.reshape(*x.shape[:-1], per_head, pair_cols)
        return jnp.moveaxis(x, 0, -2).reshape(*x.shape[1:-3], peers // 2, seqs, pair_cols)

    whole_x = jax.ShapeDtypeStruct((seqs, peers * feats), bf16)
    pieces = exchange(
        call(
            copies_kernel,
            copies,
            stream,
            specs=[held_in],
            scratch=[pltpu.VMEM(stream.shape, bf16), pltpu.SemaphoreType.DMA],
            room=MOST_VMEM,
        ),
        "tp",
    )
    got = step_of(chain, 8)
    x_local = stream
    x_full, cut = call(
        whole_kernel, (whole_x, jax.ShapeDtypeStruct((owners, seqs, rows), bf16)), pieces
    )
    seen = after((matrix_state, normalizer_state), cut)
    states = [by_piece(m) for m in seen[0]]
    normalizers = [by_piece(n) for n in seen[1]]
    everyone = exchange(cut, "dp")
    partial = call(
        partial_kernel, jax.ShapeDtypeStruct((owners, seqs, 4 * cols), bf16), everyone, own
    )
    partial = after(partial, (states, normalizers))
    parts = exchange(partial, "dp")
    chain = merged(after(chain, (partial,)), got)
    got = step_of(chain, 4)
    saved, new_stabs = ([], [])
    for block_no in range(gate_bias.shape[0]):
        if block_no == 0:
            qk, vo = call(functools.partial(sum_kernel, 2 * cols), (copies, pair), parts)
            chain = merged(after(chain, (qk,)), got)
            got = step_of(chain, 2)
        else:
            x_full, qk, vo = call(
                functools.partial(norm_kernel, 2 * cols, 4 * cols, order),
                (whole_x, copies, pair),
                pieces,
                norm_gain[:1],
                chain,
                got,
            )
            x_local = lax.dynamic_slice_in_dim(x_full, me * feats, feats, 1)
        pieces = exchange(qk, "tp")
        gate_pre = (
            jnp.dot(x_full, gate_weight[block_no], preferred_element_type=F32)
            + gate_bias[block_no]
        )
        log_in = gate_pre[:, :head_count]
        log_forget = jax.nn.log_sigmoid(gate_pre[:, head_count:])
        old_stab = stabilizer_state[block_no]
        stab_new = jnp.maximum(log_forget + old_stab, log_in)
        retain = jnp.exp(log_forget + old_stab - stab_new)
        admit = jnp.exp(log_in - stab_new)
        hidden = call(
            functools.partial(readout_kernel, head_size**-0.5),
            copies,
            pieces,
            vo,
            retain,
            admit,
            states[block_no],
            normalizers[block_no],
        )
        if block_no == 0:
            chain = merged(after(chain, (hidden,)), got)
            got = step_of(chain, 1)
        saved.append((pieces, vo, retain, admit))
        pieces = exchange(hidden, "tp")
        low = 4 * cols + block_no * feats
        summed = call(
            functools.partial(branch_kernel, cols, low, low + feats, order),
            copies,
            pieces,
            x_local,
            chain,
            got,
            scratch=[pltpu.VMEM((owners, seqs, rows), bf16)],
        )
        if block_no == 0:
            made = update(0, after(saved[0], summed), matrix_state, normalizer_state, ())
        new_stabs.append(stab_new)
        pieces = exchange(summed, "tp")
    gain = lax.dynamic_slice_in_dim(norm_gain[1:], me * feats, feats, 1)
    out = call(
        functools.partial(last_kernel, peers * feats),
        jax.ShapeDtypeStruct((seqs, feats), bf16),
        pieces,
        gain,
    )
    made = update(1, after(saved[1], (summed,)), matrix_state, normalizer_state, made)
    return (out, *made, jnp.stack(new_stabs))


def solution(mesh):
    return jax.shard_map(
        shards,
        mesh=mesh,
        in_specs=(
            P("dp", "tp"),
            P(None, "dp", "tp"),
            P(None, "dp", "tp"),
            P(None, "dp", "tp"),
            P(None, "dp", "tp"),
            P(),
            P(),
            P(None, "dp", "tp"),
            P(),
            P(None, "dp", "tp", None, None),
            P(None, "dp", None, None),
            P(None, "dp", None),
        ),
        out_specs=(
            P("dp", "tp"),
            P(None, "dp", "tp", None, None),
            P(None, "dp", None, None),
            P(None, "dp", None),
        ),
        check_vma=False,
    )
```
